128 devices in a mesh: sp: 32 (over z, y, core), tp: 4 (over x).
Axes of the slice: x: 4, y: 4, z: 4, core: 2. Of those that a mesh axis runs over, the one named last changes fastest.
Arguments:
- out_grad: bfloat16 [8192, 4096], P('sp'), may hold values from -6 to 6
- stream: bfloat16 [8192, 4096], P('sp'), may hold values from -6 to 6
- norm_gain: bfloat16 [4096], replicated, may hold values from 0.099609375 to 1.8984375
- routes: int32 [8192, 2], P('sp'), may hold values from 0 to 31, all different within a row; in each aligned block of 256 rows (0 to 255, 256 to 511, ...) at most 20 rows name the same one
- route_weight: float32 [8192, 2], P('sp'), may hold values from 0.3 to 1.5
- gate_weight: bfloat16 [32, 4096, 1024], P('sp', None, 'tp'), may hold values from -0.09375 to 0.09375
- up_weight: bfloat16 [32, 4096, 1024], P('sp', None, 'tp'), may hold values from -0.09375 to 0.09375
- down_weight: bfloat16 [32, 1024, 4096], P('sp', 'tp'), may hold values from -0.1875 to 0.1875
- out_proj: bfloat16 [4096, 1024], P(None, 'tp'), may hold values from -0.1875 to 0.1875
- conv_out: bfloat16 [8192, 1024], P('sp', 'tp'), as said below
- gate_branch: bfloat16 [8192, 1024], P('sp', 'tp'), may hold values from -6 to 6
- decay_map: bfloat16 [2, 4, 256, 256], P(None, 'tp'), as said below
- input_map: bfloat16 [2, 4, 256, 256], P(None, 'tp'), as said below
- decay_param: float32 [2, 1024], P(None, 'tp'), as said below
- decay_shift: float32 [2, 8192, 1024], P(None, 'sp', 'tp'), as said below
- states: float32 [2, 8192, 1024], P(None, 'sp', 'tp'), as said below
Outputs:
- conv_grad: float32 [8192, 1024], P('sp', 'tp')
- gate_branch_grad: float32 [8192, 1024], P('sp', 'tp')
- out_proj_grad: float32 [4096, 1024], P('sp', 'tp')
- gate_weight_grad: bfloat16 [32, 4096, 1024], P('sp', None, 'tp')
- up_weight_grad: bfloat16 [32, 4096, 1024], P('sp', None, 'tp')
- down_weight_grad: bfloat16 [32, 1024, 4096], P('sp', 'tp')
The draws below stay inside these ranges and needn't reach their ends.
Inputs may be any that keep to these rules, and one draw needn't show every extreme that they name: `routes`: each token names 2 different experts. Among the 256 tokens of one index of sp no expert is named more than 20 times, a bound that some expert reaches in some of these blocks. `conv_out`: within -6 to 6. `decay_map`: entries within -4 to 4 times 256 to the power -0.5. `input_map`: entries within -4 to 4 times 256 to the power -0.5. `decay_param`: between 3.7 and 3.5 plus the logarithm of 8192. `decay_shift`: every entry lies between -0.7 and -0.00002. The forward pass's states: they follow the recurrences of the steps from conv_out, decay_map, input_map, decay_param and decay_shift.
All inputs are finite; a program needn't handle non-finite values.
Results may differ from the reference program's by a relative error of at most 0.018.
Values may be sent and summed in bfloat16 or wider, within the bound.
No kernel may reach another device: no remote copies, remote signals or barrier semaphores. Data moves between devices by JAX's collectives and lax.ppermute only.
A program may use at most 128 MiB of HBM per device.

```python
import math
import jax
import jax.numpy as jnp
import numpy as np
from jax import lax

D = 4096
RECURRENT_WIDTH = 1024
BLOCKS = 4
BW = 256
FF = 1024
TOP = 2
TOK_DEV = 256
EXPERTS = 32
SEQUENCE_TOKENS = 8192
CAP = 20
N_SP = 32
N_TP = 4


def scan_pairs(coeffs, values, reverse):

    def combine(earlier, later):
        return (earlier[0] * later[0], later[0] * earlier[1] + later[1])
    return lax.associative_scan(combine, (coeffs, values), axis=0, reverse=reverse)[1]


def block_apply(channels, block_maps):
    shaped = channels.reshape(channels.shape[0], block_maps.shape[0], block_maps.shape[1])
    mapped = jnp.einsum('tkc,kcd->tkd', shaped, block_maps.astype(jnp.float32), precision=lax.Precision.HIGHEST)
    return mapped.reshape(channels.shape)


def lru_draw(key):
    random_keys = jax.random.split(jax.random.fold_in(key, 4242), 9)
    conv_field = jax.random.normal(random_keys[1], (SEQUENCE_TOKENS, RECURRENT_WIDTH), jnp.float32)
    fast_share = 0.5
    conv_field = jnp.clip(conv_field, -6.0, 6.0).astype(jnp.bfloat16)
    gate_maps = jnp.clip(jax.random.normal(random_keys[2], (2, 2, BLOCKS, BW, BW), jnp.float32), -4.0, 4.0)
    gate_maps = (gate_maps * BW ** (-0.5)).astype(jnp.bfloat16)
    fast_mask = jax.random.uniform(random_keys[3], (2, RECURRENT_WIDTH), jnp.float32) < fast_share
    slow_values = jnp.log(SEQUENCE_TOKENS * 1.0) + jax.random.uniform(random_keys[4], (2, RECURRENT_WIDTH), jnp.float32, 2.0, 3.5)
    fast_values = jax.random.uniform(random_keys[5], (2, RECURRENT_WIDTH), jnp.float32, 3.7, 4.9)
    decay_values = jnp.where(fast_mask, fast_values, slow_values)
    block_count = SEQUENCE_TOKENS // TOK_DEV
    block_rate = jnp.exp(jax.random.uniform(random_keys[6], (2, block_count), jnp.float32, -10.6, -9.2))
    shift_offset = -jnp.repeat(block_rate, TOK_DEV, axis=1)[:, :, None]
    spike_mask = jax.random.uniform(random_keys[7], (2, SEQUENCE_TOKENS, RECURRENT_WIDTH), jnp.float32) < 1.5 / SEQUENCE_TOKENS
    spike_depth = jnp.log(jax.random.uniform(random_keys[8], (2, SEQUENCE_TOKENS, RECURRENT_WIDTH), jnp.float32, 0.5, 0.8))
    offset_field = shift_offset + jnp.where(spike_mask, spike_depth, 0.0)
    conv_float = conv_field.astype(jnp.float32)
    state_list = []
    for direction in range(2):
        decay_gate = jax.nn.sigmoid(block_apply(conv_float, gate_maps[0, direction]))
        input_gate = jax.nn.sigmoid(block_apply(conv_float, gate_maps[1, direction]))
        log_decay = -8.0 * decay_gate * jax.nn.softplus(-decay_values[direction])[None, :] + offset_field[direction]
        drive_term = jnp.sqrt(-jnp.expm1(2.0 * log_decay)) * input_gate * conv_float
        state_list.append(scan_pairs(jnp.exp(log_decay), drive_term, direction == 1))
    return (conv_field, gate_maps[0], gate_maps[1], decay_values, offset_field, jnp.stack(state_list))


def draw_conv_out(key, part):
    return lru_draw(key)[0]


def draw_decay_map(key, part):
    return lru_draw(key)[1]


def draw_input_map(key, part):
    return lru_draw(key)[2]


def draw_decay_param(key, part):
    return lru_draw(key)[3]


def draw_decay_shift(key, part):
    return lru_draw(key)[4]


def draw_states(key, part):
    return lru_draw(key)[5]


def raised(values, rng, source, target, blocks, factor):
    owner, partner = [(jnp.arange(values.shape[position]) // (values.shape[position] // blocks)).reshape([-1 if axis == position else 1 for axis in range(values.ndim)]) for position in (source, target)]
    chosen = jax.random.permutation(rng, blocks)[partner]
    strong = (owner == chosen) | (owner == (partner + blocks // 2) % blocks)
    return jnp.where(strong, factor * values, values)


def levels(key, dims, pieces, least, largest):
    loudness = 1.0
    for position, parts in pieces:
        heights = jax.random.uniform(jax.random.fold_in(jax.random.fold_in(key, 6), position), (parts,), jnp.float32, least / len(pieces), largest / len(pieces))
        loudness = loudness * jnp.repeat(jnp.exp(heights), dims[position] // parts).reshape((-1,) + (1,) * (len(dims) - 1 - position))
    return loudness


def deal_out(key, own, number, rows, number_of, top, most, lean):
    order = jax.random.permutation(key, number_of)
    crowded, common = load_shares(number_of, rows * top, most, lean, True), load_shares(number_of, rows * top, most, lean, False)
    places = jnp.arange(number_of)

    def named(tallies, offset_by):
        used = int((tallies > 0).sum())
        fixed = max(1, used // 4)
        shifted = fixed + (places - fixed + offset_by * (used - fixed)) % max(1, number_of - fixed)
        return jnp.zeros((number_of,), jnp.int32).at[order[jnp.where(places < fixed, places, shifted)]].set(jnp.asarray(tallies, jnp.int32))

    tallies = jnp.where(number % 4 == 0, named(crowded, number // 4), named(common, number - number // 4 - 1))
    mixed = jax.random.permutation(jax.random.fold_in(own, 3), number_of)
    donor, sink = mixed[0:number_of // 2 * 2:2], mixed[1:number_of // 2 * 2:2]
    room = jnp.minimum(tallies[donor] - 1, most - tallies[sink]) // 2
    room = jnp.where((donor == order[0]) | (sink == order[0]) | (tallies[sink] == 0), 0, jnp.maximum(room, 0))
    shifted = jax.random.randint(jax.random.fold_in(own, 4), (number_of // 2,), 0, 1 << 20) % (room + 1)
    tallies = tallies.at[donor].add(-shifted).at[sink].add(shifted)
    members = jnp.searchsorted(jnp.cumsum(tallies), jnp.arange(rows * top), side="right").astype(jnp.int32)
    grid = members.reshape(top, rows).T
    grid = grid[jax.random.permutation(jax.random.fold_in(own, 1), rows)]
    offset_by = jax.random.randint(jax.random.fold_in(own, 2), (rows, 1), 0, top)
    return jnp.take_along_axis(grid, (jnp.arange(top)[None, :] + offset_by) % top, axis=1)


def load_shares(count, total, limit, skew, full):
    loads = [(1 << 20) // math.isqrt(standing ** skew) + 1 for standing in range(1, count + 1)]
    largest = limit if full else min(limit, max(-(-total // count), total * loads[0] // sum(loads)))
    least = 1 if total - largest >= count - 1 else 0
    counts, rest = [largest] + [least] * (count - 1), total - largest - least * (count - 1)
    while rest > 0:
        movable = [i for i in range(1, count) if counts[i] < largest] or [i for i in range(1, count) if counts[i] < limit]
        whole, remaining = sum([loads[i] for i in movable]), rest
        for i in movable:
            more = min(limit - counts[i], max(1, remaining * loads[i] // whole), rest)
            counts[i] = counts[i] + more
            rest = rest - more
    return np.array(counts)


def bell_draw(stream_key, shape, deviation, reach, shards=(), held_as=jnp.bfloat16):
    drawn = deviation * jax.random.normal(stream_key, shape, jnp.float32)
    if shards:
        drawn = drawn * levels(stream_key, shape, shards, -0.22, 0.18)
    return jnp.clip(drawn, -reach, reach).astype(held_as)


def noise_with(own_key, dims, deviation, most, cuts, heavy, kind=jnp.bfloat16):
    array = deviation * jax.random.normal(own_key, dims, jnp.float32)
    if cuts:
        array = array * levels(own_key, dims, cuts, -0.22, 0.18)
    return jnp.clip(raised(array, jax.random.fold_in(own_key, 3), *heavy), -most, most).astype(kind)


def setup_inputs(seed: int = 0) -> dict:
    key_of = jax.random.split(jax.random.key(seed), 17)
    out_grad = noise_with(key_of[0], (SEQUENCE_TOKENS, D), 1.0, 6.0, ((0, 32),), (0, 1, 32, 2.75))
    stream = bell_draw(key_of[1], (SEQUENCE_TOKENS, D), 1.0, 6.0, ((0, 32),))
    norm_gain = jnp.clip(1.0 + 0.18 * jax.random.normal(key_of[2], (D,), jnp.float32), 0.099609375, 1.8984375).astype(jnp.bfloat16)
    routes_keys = jax.random.split(jax.random.fold_in(key_of[3], 1), SEQUENCE_TOKENS // TOK_DEV)
    routes_turns = jax.random.permutation(jax.random.fold_in(key_of[3], 3), SEQUENCE_TOKENS // TOK_DEV)
    routes = jax.vmap(lambda own, number: deal_out(jax.random.fold_in(key_of[3], 2), own, number, TOK_DEV, EXPERTS, TOP, CAP, 1))(routes_keys, routes_turns).reshape((SEQUENCE_TOKENS, TOP))
    route_weight = jnp.clip(0.3 + 1.2 * jax.random.uniform(key_of[4], (SEQUENCE_TOKENS, TOP), jnp.float32) ** levels(key_of[4], (SEQUENCE_TOKENS, TOP), ((0, 32),), -0.2, 0.2), 0.3, 1.5)
    gate_weight = bell_draw(key_of[5], (EXPERTS, D, FF), D ** -0.5, 0.09375, ((0, 32), (2, 4)))
    up_weight = bell_draw(key_of[6], (EXPERTS, D, FF), D ** -0.5, 0.09375, ((0, 32), (2, 4)))
    down_weight = bell_draw(key_of[7], (EXPERTS, FF, D), FF ** -0.5, 0.1875, ((0, 32), (1, 4)))
    out_proj = bell_draw(key_of[8], (D, RECURRENT_WIDTH), RECURRENT_WIDTH ** -0.5, 0.1875, ((1, 4),))
    conv_out = draw_conv_out(jax.random.fold_in(key_of[16], 71), 0)
    gate_branch = bell_draw(key_of[10], (SEQUENCE_TOKENS, RECURRENT_WIDTH), 1.0, 6.0, ((0, 32), (1, 4)))
    decay_map = draw_decay_map(jax.random.fold_in(key_of[16], 71), 0)
    input_map = draw_input_map(jax.random.fold_in(key_of[16], 71), 0)
    decay_param = draw_decay_param(jax.random.fold_in(key_of[16], 71), 0)
    decay_shift = draw_decay_shift(jax.random.fold_in(key_of[16], 71), 0)
    states = draw_states(jax.random.fold_in(key_of[16], 71), 0)
    return dict(out_grad=out_grad, stream=stream, norm_gain=norm_gain, routes=routes, route_weight=route_weight, gate_weight=gate_weight, up_weight=up_weight, down_weight=down_weight, out_proj=out_proj, conv_out=conv_out, gate_branch=gate_branch, decay_map=decay_map, input_map=input_map, decay_param=decay_param, decay_shift=decay_shift, states=states)


rate_scale = 8.0
norm_eps = 1e-06

def contract(left, right, left_dim, right_dim):
    return lax.dot_general(left, right, (((left_dim,), (right_dim,)), ((), ())), preferred_element_type=jnp.float32)

def linear_scan(coeffs, values, reverse):

    def combine(earlier, later):
        return (earlier[0] * later[0], later[0] * earlier[1] + later[1])
    return lax.associative_scan(combine, (coeffs, values), axis=0, reverse=reverse)

def silu_grad(values):
    logistic = jax.nn.sigmoid(values)
    return logistic * (1.0 + values * (1.0 - logistic))

def expert_pass(slot_inputs, slot_cotan, gate_local, up_local, down_local):
    gate_pre = contract(slot_inputs, gate_local, 1, 0)
    up_pre = contract(slot_inputs, up_local, 1, 0)
    hidden = (jax.nn.silu(gate_pre) * up_pre).astype(jnp.bfloat16)
    down_wgrad = contract(hidden, slot_cotan, 0, 0)
    hidden_grad = contract(slot_cotan, down_local, 1, 1)
    up_grad = (hidden_grad * jax.nn.silu(gate_pre)).astype(jnp.bfloat16)
    gate_grad = (hidden_grad * up_pre * silu_grad(gate_pre)).astype(jnp.bfloat16)
    gate_wgrad = contract(slot_inputs, gate_grad, 0, 0)
    up_wgrad = contract(slot_inputs, up_grad, 0, 0)
    return (gate_wgrad, up_wgrad, down_wgrad, gate_grad, up_grad)

def block_forward(channels, block_maps):
    shaped = channels.reshape(channels.shape[0], block_maps.shape[0], block_maps.shape[1])
    mapped = jnp.einsum('tkc,kcd->tkd', shaped, block_maps.astype(jnp.float32), precision=lax.Precision.HIGHEST)
    return mapped.reshape(channels.shape)

def block_backward(pre_grad, block_maps):
    shaped = pre_grad.reshape(pre_grad.shape[0], block_maps.shape[0], block_maps.shape[2])
    mapped = jnp.einsum('tkd,kcd->tkc', shaped, block_maps.astype(jnp.float32), precision=lax.Precision.HIGHEST)
    return mapped.reshape(pre_grad.shape)

def recurrence_back(adjoint, state_run, conv_float, gate_parts, decay_local, input_local):
    decay_gate, input_gate, decay_base, decay_rate, drive_scale, drive_term = gate_parts
    log_grad = adjoint * (state_run - drive_term) - adjoint * input_gate * conv_float * decay_rate * decay_rate / drive_scale
    decay_pre_grad = log_grad * (-rate_scale * decay_base) * decay_gate * (1.0 - decay_gate)
    input_pre_grad = adjoint * drive_scale * conv_float * input_gate * (1.0 - input_gate)
    return adjoint * drive_scale * input_gate + block_backward(decay_pre_grad, decay_local) + block_backward(input_pre_grad, input_local)

def reference(out_grad, stream, norm_gain, routes, route_weight, gate_weight, up_weight, down_weight, out_proj, conv_out, gate_branch, decay_map, input_map, decay_param, decay_shift, states):
    stream_f = stream.astype(jnp.float32)
    row_scale = lax.rsqrt(lax.optimization_barrier(jnp.mean(stream_f * stream_f, axis=1, keepdims=True)) + norm_eps)
    unit_rows = stream_f * row_scale
    gain_row = norm_gain.astype(jnp.float32)[None, :]
    normed = (unit_rows * gain_row).astype(jnp.bfloat16)
    pair_count = SEQUENCE_TOKENS * TOP
    pair_expert = routes.reshape(N_SP, TOK_DEV * TOP)
    onehot = (pair_expert[:, :, None] == jnp.arange(EXPERTS, dtype=jnp.int32)[None, None, :]).astype(jnp.int32)
    slot_rank = lax.optimization_barrier(jnp.sum((jnp.cumsum(onehot, axis=1) - onehot) * onehot, axis=2))
    source = jnp.arange(N_SP, dtype=jnp.int32)[:, None]
    slot_index = (pair_expert * (N_SP * CAP) + source * CAP + slot_rank).reshape(-1).astype(jnp.int32)
    slot_pair = jnp.full((EXPERTS * N_SP * CAP,), pair_count, jnp.int32).at[slot_index].set(jnp.arange(pair_count, dtype=jnp.int32))
    slot_token = (slot_pair // TOP).astype(jnp.int32)
    zero_row = jnp.zeros((1, D), jnp.bfloat16)
    slot_inputs = jnp.concatenate([normed, zero_row])[slot_token].reshape(EXPERTS, N_SP * CAP, D)
    weight_pad = jnp.concatenate([route_weight.reshape(-1), jnp.zeros((1,), jnp.float32)])
    slot_cotan = (weight_pad[slot_pair][:, None] * jnp.concatenate([out_grad, zero_row])[slot_token].astype(jnp.float32)).astype(jnp.bfloat16)
    slot_cotan = slot_cotan.reshape(EXPERTS, N_SP * CAP, D)

    def one_expert(operands):
        inputs_e, cotan_e, gate_local, up_local, down_local = operands
        gate_wgrad, up_wgrad, down_wgrad, gate_grad, up_grad = expert_pass(inputs_e, cotan_e, gate_local, up_local, down_local)
        run_width = FF // N_TP
        total_sum = jnp.zeros((inputs_e.shape[0], D), jnp.float32)
        for quarter in range(N_TP):
            low_unit = quarter * run_width
            high_unit = low_unit + run_width
            partial_value = contract(gate_grad[:, low_unit:high_unit], gate_local[:, low_unit:high_unit], 1, 1) + contract(up_grad[:, low_unit:high_unit], up_local[:, low_unit:high_unit], 1, 1)
            total_sum = total_sum + lax.optimization_barrier(partial_value.astype(jnp.bfloat16)).astype(jnp.float32)
        return (gate_wgrad.astype(jnp.bfloat16), up_wgrad.astype(jnp.bfloat16), down_wgrad.astype(jnp.bfloat16), total_sum.astype(jnp.bfloat16))
    gate_grads, up_grads, down_grads, pair_grad = lax.map(one_expert, (slot_inputs, slot_cotan, gate_weight, up_weight, down_weight))
    returned = pair_grad.reshape(EXPERTS * N_SP * CAP, D)[slot_index]
    normed_grad = lax.optimization_barrier(jnp.sum(returned.reshape(SEQUENCE_TOKENS, TOP, D).astype(jnp.float32), axis=1))
    scaled_grad = gain_row * normed_grad
    stream_grad = out_grad.astype(jnp.float32) + row_scale * (scaled_grad - unit_rows * lax.optimization_barrier(jnp.mean(unit_rows * scaled_grad, axis=1, keepdims=True)))
    stream_grad_b = stream_grad.astype(jnp.bfloat16)
    total_state = states[0] + states[1]
    gate_float = gate_branch.astype(jnp.float32)
    gelu_gate, gelu_back = jax.vjp(jax.nn.gelu, gate_float)
    lru_out = (total_state * gelu_gate).astype(jnp.bfloat16)
    out_proj_grad = contract(stream_grad_b, lru_out, 0, 0)
    lru_out_grad = contract(stream_grad_b, out_proj, 1, 0)
    gate_branch_grad = gelu_back(lru_out_grad * total_state)[0]
    state_grad = lru_out_grad * gelu_gate
    conv_float = conv_out.astype(jnp.float32)
    ones_row = jnp.ones((1, RECURRENT_WIDTH), jnp.float32)
    conv_grad = jnp.zeros_like(conv_float)
    for direction in range(2):
        decay_gate = jax.nn.sigmoid(block_forward(conv_float, decay_map[direction]))
        input_gate = jax.nn.sigmoid(block_forward(conv_float, input_map[direction]))
        decay_base = jax.nn.softplus(-decay_param[direction])[None, :]
        log_decay = -rate_scale * decay_gate * decay_base + decay_shift[direction]
        decay_rate = jnp.exp(log_decay)
        drive_scale = jnp.sqrt(-jnp.expm1(2.0 * log_decay))
        drive_term = drive_scale * input_gate * conv_float
        if direction == 0:
            adjoint = linear_scan(jnp.concatenate([decay_rate[1:], ones_row]), state_grad, True)[1]
        else:
            adjoint = linear_scan(jnp.concatenate([ones_row, decay_rate[:-1]]), state_grad, False)[1]
        gate_parts = (decay_gate, input_gate, decay_base, decay_rate, drive_scale, drive_term)
        conv_grad = conv_grad + recurrence_back(adjoint, states[direction], conv_float, gate_parts, decay_map[direction], input_map[direction])
    return (conv_grad, gate_branch_grad, out_proj_grad, gate_grads, up_grads, down_grads)
```

```python
import functools

import jax
import jax.numpy as jnp
from jax import lax
from jax.experimental import pallas as pl
from jax.experimental.pallas import tpu as pltpu
from jax.sharding import Mesh
from jax.sharding import PartitionSpec as P

TOP = 2
SP = ("sp_0", "sp_1", "sp_2")
BF = jnp.bfloat16
F32 = jnp.float32

rate_scale = 8.0
norm_eps = 1e-06


def contract(left, right, left_dim, right_dim):
    return lax.dot_general(
        left, right, (((left_dim,), (right_dim,)), ((), ())), preferred_element_type=F32
    )


def shifted(x, axis, k):
    n = lax.axis_size(axis)
    return lax.ppermute(x, axis, [(i, (i + k) % n) for i in range(n)])


def vmem():
    return pl.BlockSpec(memory_space=pltpu.MemorySpace.VMEM)


def prep_kernel(
    q_ref, stream_ref, stream_q_ref, cotan_ref, gain_ref, routes_ref, weight_ref,
    inputs_ref, slots_ref, scale_ref, index_ref, *, experts, capacity,
):
    tokens, width = stream_ref.shape
    slots = experts * capacity
    whole = stream_ref[...].astype(F32)
    scale = lax.rsqrt(jnp.sum(whole * whole, axis=1, keepdims=True) * (1.0 / width) + norm_eps)
    scale_ref[...] = scale
    normed = (stream_q_ref[...].astype(F32) * scale * gain_ref[...].astype(F32)).astype(BF)
    expert = lax.broadcasted_iota(jnp.int32, (experts, tokens), 0)
    hits = [jnp.where(expert == routes_ref[k : k + 1, :], 1.0, 0.0) for k in range(TOP)]
    before = jnp.where(
        lax.broadcasted_iota(jnp.int32, (tokens, tokens), 0)
        < lax.broadcasted_iota(jnp.int32, (tokens, tokens), 1),
        1.0,
        0.0,
    ).astype(BF)
    earlier = jnp.dot((hits[0] + hits[1]).astype(BF), before, preferred_element_type=F32)
    place = lax.broadcasted_iota(jnp.int32, (slots, tokens), 0)
    picks = []
    for k in range(TOP):
        rank = jnp.sum(earlier * hits[k], axis=0, keepdims=True).astype(jnp.int32)
        slot = routes_ref[k : k + 1, :] * capacity + rank
        index_ref[k : k + 1, :] = slot
        picks.append(jnp.where(place == slot, 1.0, 0.0))
    inputs_ref[...] = jnp.dot(
        (picks[0] + picks[1]).astype(BF), normed, preferred_element_type=F32
    ).astype(BF)
    cotan = cotan_ref[...].astype(F32)
    total = 0.0
    for k in range(TOP):
        scaled = (weight_ref[:, k : k + 1] * cotan).astype(BF)
        total = total + jnp.dot(picks[k].astype(BF), scaled, preferred_element_type=F32)
    slots_ref[...] = total.astype(BF)


def prep(q, stream, out_grad, gain, routes_t, weight, experts, capacity):
    tokens, width = stream.shape
    quarter = width // 4
    slots = experts * capacity
    full = lambda shape: pl.BlockSpec(shape, lambda i, q_ref: (0, 0))
    part = lambda rows: pl.BlockSpec((rows, quarter), lambda i, q_ref: (0, q_ref[0]))
    return pl.pallas_call(
        functools.partial(prep_kernel, experts=experts, capacity=capacity),
        grid_spec=pltpu.PrefetchScalarGridSpec(
            num_scalar_prefetch=1,
            grid=(1,),
            in_specs=[
                full((tokens, width)),
                part(tokens),
                part(tokens),
                part(1),
                full((8, tokens)),
                full((tokens, TOP)),
            ],
            out_specs=[
                full((slots, quarter)),
                full((slots, quarter)),
                full((tokens, 1)),
                full((8, tokens)),
            ],
        ),
        out_shape=[
            jax.ShapeDtypeStruct((slots, quarter), BF),
            jax.ShapeDtypeStruct((slots, quarter), BF),
            jax.ShapeDtypeStruct((tokens, 1), F32),
            jax.ShapeDtypeStruct((8, tokens), jnp.int32),
        ],
        name="prep",
    )(q, stream, stream, out_grad, gain, routes_t, weight)


def combine_kernel(q_ref, back_ref, index_ref, stream_ref, scale_ref, gain_ref, grad_ref, part_ref):
    slots = back_ref.shape[0]
    tokens = stream_ref.shape[0]
    place = lax.broadcasted_iota(jnp.int32, (slots, tokens), 0)
    pick = jnp.where(
        (place == index_ref[0:1, :]) | (place == index_ref[1:2, :]), 1.0, 0.0
    ).astype(BF)
    normed_grad = lax.dot_general(
        pick, back_ref[...], (((0,), (0,)), ((), ())), preferred_element_type=F32
    )
    scaled_grad = gain_ref[...].astype(F32) * normed_grad
    grad_ref[...] = scaled_grad
    unit = stream_ref[...].astype(F32) * scale_ref[...]
    part = jnp.sum(unit * scaled_grad, axis=1, keepdims=True)
    part_ref[...] = jnp.broadcast_to(part, (tokens, 128)).T[:8]


def combine(q, back, index, stream, scale, gain):
    slots, quarter = back.shape
    tokens = stream.shape[0]
    full = lambda shape: pl.BlockSpec(shape, lambda i, q_ref: (0, 0))
    part = lambda rows: pl.BlockSpec((rows, quarter), lambda i, q_ref: (0, q_ref[0]))
    return pl.pallas_call(
        combine_kernel,
        grid_spec=pltpu.PrefetchScalarGridSpec(
            num_scalar_prefetch=1,
            grid=(1,),
            in_specs=[
                full((slots, quarter)),
                full((8, tokens)),
                part(tokens),
                full((tokens, 1)),
                part(1),
            ],
            out_specs=[full((tokens, quarter)), full((8, tokens))],
        ),
        out_shape=[
            jax.ShapeDtypeStruct((tokens, quarter), F32),
            jax.ShapeDtypeStruct((8, tokens), F32),
        ],
        name="combine",
    )(q, back, index, stream, scale, gain)


def stream_kernel(
    q_ref, t0_ref, t1_ref, t2_ref, t3_ref, grad_ref, stream_ref, cotan_ref, scale_ref,
    p0_ref, p1_ref, p2_ref, p3_ref, sgb_ref, b0_ref, b1_ref, b2_ref, b3_ref, *, width,
):
    total = (t0_ref[...] + t1_ref[...]) + (t2_ref[...] + t3_ref[...])
    column = jnp.concatenate([total] * 16, axis=0).T[:, :1]
    mean = column * (1.0 / width)
    scale = scale_ref[...]
    unit = stream_ref[...].astype(F32) * scale
    grad = cotan_ref[...].astype(F32) + scale * (grad_ref[...] - unit * mean)
    grad_b = grad.astype(BF)
    sgb_ref[...] = grad_b
    for p_ref, b_ref in ((p1_ref, b1_ref), (p2_ref, b2_ref), (p3_ref, b3_ref), (p0_ref, b0_ref)):
        b_ref[...] = jnp.dot(grad_b, p_ref[...], preferred_element_type=F32).astype(b_ref.dtype)


def stream_back(q, totals, grad, stream, out_grad, scale, projs):
    tokens, quarter = grad.shape
    channels = projs[0].shape[1]
    full = lambda shape: pl.BlockSpec(shape, lambda i, q_ref: (0, 0))
    part = lambda rows: pl.BlockSpec((rows, quarter), lambda i, q_ref: (0, q_ref[0]))
    return pl.pallas_call(
        functools.partial(stream_kernel, width=stream.shape[1]),
        grid_spec=pltpu.PrefetchScalarGridSpec(
            num_scalar_prefetch=1,
            grid=(1,),
            in_specs=[full((8, tokens))] * 4
            + [full((tokens, quarter)), part(tokens), part(tokens), full((tokens, 1))]
            + [full((quarter, channels))] * 4,
            out_specs=[full((tokens, quarter))] + [full((tokens, channels))] * 4,
        ),
        out_shape=[jax.ShapeDtypeStruct((tokens, quarter), BF)]
        + [jax.ShapeDtypeStruct((tokens, channels), F32)]
        + [jax.ShapeDtypeStruct((tokens, channels), BF)] * 3,
        name="stream_back",
    )(q, *totals, grad, stream, out_grad, scale, *projs)


CHUNKS = 8


def scan_kernel(
    b0_ref, b1_ref, b2_ref, b3_ref, gate_mul_ref, gelu_ref, decay_ref, shift_ref,
    branch_ref, inner_ref, reach_ref, summary_ref, state_ref,
):
    tokens, channels = gelu_ref.shape
    length = tokens // CHUNKS
    out_grad = b0_ref[...] + (
        b1_ref[...].astype(F32) + b2_ref[...].astype(F32) + b3_ref[...].astype(F32)
    )
    branch_ref[...] = out_grad * gate_mul_ref[...]
    state_ref[...] = out_grad * gelu_ref[...]
    zero = jnp.zeros((CHUNKS, channels), F32)
    one = jnp.ones((CHUNKS, channels), F32)

    def step(i, carry):
        sum_0, mul_0, sum_1, mul_1 = carry
        at_0 = pl.ds(length - 1 - i, CHUNKS, stride=length)
        at_1 = pl.ds(i, CHUNKS, stride=length)
        coeff_0 = shift_ref[0, at_0, :]
        coeff_1 = shift_ref[1, at_1, :]
        sum_0 = state_ref[at_0, :] + coeff_0 * sum_0
        sum_1 = state_ref[at_1, :] + coeff_1 * sum_1
        mul_0 = coeff_0 * mul_0
        mul_1 = coeff_1 * mul_1
        inner_ref[0, at_0, :] = sum_0
        inner_ref[1, at_1, :] = sum_1
        reach_ref[0, at_0, :] = mul_0
        reach_ref[1, at_1, :] = mul_1
        return (sum_0, mul_0, sum_1, mul_1)

    lax.fori_loop(0, length, step, (zero, one, zero, one), unroll=4)
    row_sum = jnp.zeros((1, channels), F32)
    row_mul = jnp.ones((1, channels), F32)
    for s in reversed(range(CHUNKS)):
        at = s * length
        row_sum = inner_ref[0, at : at + 1, :] + reach_ref[0, at : at + 1, :] * row_sum
        row_mul = reach_ref[0, at : at + 1, :] * row_mul
    last = decay_ref[0, 0:1, :]
    summary_ref[0:1, :] = last * row_mul
    summary_ref[1:2, :] = last * row_sum
    row_sum = jnp.zeros((1, channels), F32)
    row_mul = jnp.ones((1, channels), F32)
    for s in range(CHUNKS):
        at = s * length + length - 1
        row_sum = inner_ref[1, at : at + 1, :] + reach_ref[1, at : at + 1, :] * row_sum
        row_mul = reach_ref[1, at : at + 1, :] * row_mul
    last = decay_ref[1, tokens - 1 : tokens, :]
    summary_ref[2:3, :] = last * row_mul
    summary_ref[3:4, :] = last * row_sum
    summary_ref[4:8, :] = jnp.zeros((4, channels), F32)


def scan_back(blocks, gate_mul, gelu_gate, decay, shift):
    tokens, channels = gelu_gate.shape
    lanes = 128
    flat = pl.BlockSpec((tokens, lanes), lambda i: (0, i))
    both = pl.BlockSpec((2, tokens, lanes), lambda i: (0, 0, i))
    return pl.pallas_call(
        scan_kernel,
        grid=(channels // lanes,),
        in_specs=[flat] * 6 + [both] * 2,
        out_specs=[flat, both, both, pl.BlockSpec((8, lanes), lambda i: (0, i))],
        out_shape=[
            jax.ShapeDtypeStruct((tokens, channels), F32),
            jax.ShapeDtypeStruct((2, tokens, channels), F32),
            jax.ShapeDtypeStruct((2, tokens, channels), F32),
            jax.ShapeDtypeStruct((8, channels), F32),
        ],
        scratch_shapes=[pltpu.VMEM((tokens, lanes), F32)],
        name="scan_back",
    )(*blocks, gate_mul, gelu_gate, decay, shift)


def split_dot(value, map_ref):
    high = value.astype(BF)
    low = (value - high.astype(F32)).astype(BF)
    dims = (((1,), (1,)), ((), ()))
    return lax.dot_general(high, map_ref, dims, preferred_element_type=F32) + lax.dot_general(
        low, map_ref, dims, preferred_element_type=F32
    )


def final_kernel(
    at_ref, g0_ref, g1_ref, g2_ref, g3_ref, inner_ref, reach_ref, direct_ref, decay_mul_ref,
    input_mul_ref, decay_map_ref, input_map_ref, out_ref, adjoint_ref,
):
    tokens, channels = out_ref.shape
    length = tokens // CHUNKS
    z, y, c = at_ref[0], at_ref[1], at_ref[2]
    mine = z * 8 + y * 2 + c
    refs = (g0_ref, g1_ref, g2_ref, g3_ref)
    from_right = jnp.zeros((1, channels), F32)
    from_left = jnp.zeros((1, channels), F32)

    def piece(k):
        dz = lax.rem(k // 8 - z + 4, 4)
        dy = lax.rem(lax.rem(k // 2, 4) - y + 4, 4)
        dc = lax.rem(lax.rem(k, 2) - c + 2, 2)
        row = dy * 2 + dc
        tile = jnp.where(dz == 0, refs[0][row], jnp.where(dz == 1, refs[1][row], jnp.where(dz == 2, refs[2][row], refs[3][row])))
        return tile

    for k in range(31):
        right = 31 - k
        tile = piece(right)
        from_right = jnp.where(right > mine, tile[1:2] + tile[0:1] * from_right, from_right)
        tile = piece(k)
        from_left = jnp.where(k < mine, tile[3:4] + tile[2:3] * from_left, from_left)
    carry = from_right
    for s in reversed(range(CHUNKS)):
        rows = slice(s * length, s * length + length)
        adjoint_ref[0, rows, :] = inner_ref[0, rows, :] + reach_ref[0, rows, :] * carry
        carry = adjoint_ref[0, s * length : s * length + 1, :]
    carry = from_left
    for s in range(CHUNKS):
        rows = slice(s * length, s * length + length)
        adjoint_ref[1, rows, :] = inner_ref[1, rows, :] + reach_ref[1, rows, :] * carry
        carry = adjoint_ref[1, s * length + length - 1 : s * length + length, :]
    total = jnp.zeros((tokens, channels), F32)
    for d in range(2):
        adjoint = adjoint_ref[d]
        total = total + adjoint * direct_ref[d]
        total = total + split_dot(adjoint * decay_mul_ref[d], decay_map_ref[d])
        total = total + split_dot(adjoint * input_mul_ref[d], input_map_ref[d])
    out_ref[...] = total


def final_back(at, gathered, inner, reach, direct, decay_mul, input_mul, decay_map, input_map):
    _, tokens, channels = inner.shape
    return pl.pallas_call(
        final_kernel,
        in_specs=[pl.BlockSpec(memory_space=pltpu.MemorySpace.SMEM)] + [vmem()] * 11,
        out_specs=vmem(),
        out_shape=jax.ShapeDtypeStruct((tokens, channels), F32),
        scratch_shapes=[pltpu.VMEM((2, tokens, channels), F32)],
        name="final_back",
    )(at, *gathered, inner, reach, direct, decay_mul, input_mul, decay_map, input_map)


def silu_grad(values):
    logistic = jax.nn.sigmoid(values)
    return logistic * (1.0 + values * (1.0 - logistic))


def body(
    out_grad,
    stream,
    norm_gain,
    routes,
    route_weight,
    gate_weight,
    up_weight,
    down_weight,
    out_proj,
    conv_out,
    gate_branch,
    decay_map,
    input_map,
    decay_param,
    decay_shift,
    states,
):
    sources = lax.axis_size(SP)
    experts = sources
    token_count, model_width = stream.shape
    capacity = (5 * TOP * token_count + 4 * experts - 1) // (4 * experts)
    slots = sources * capacity
    half = slots // 2
    width = model_width // 4
    q = lax.axis_index("tp")
    z, y, c = (lax.axis_index(a) for a in SP)
    q_arr = q.astype(jnp.int32).reshape(1)
    gate_w, up_w, down_w = gate_weight[0], up_weight[0], down_weight[0]
    units = gate_w.shape[1]
    channels = out_proj.shape[1]
    gain = norm_gain[None, :]

    def rows_of(array, k):
        return lax.dynamic_slice_in_dim(array, (k % 4) * width, width, 0)

    def cols_of(array, k):
        return lax.dynamic_slice_in_dim(array, (k % 4) * width, width, 1)

    down_rel = [cols_of(down_w, q)] + [
        shifted(cols_of(down_w, q + 4 - j), "tp", -j) for j in (1, 2, 3)
    ]
    proj_rel = [rows_of(out_proj, q)] + [
        shifted(rows_of(out_proj, q + 4 - j), "tp", -j) for j in (1, 2, 3)
    ]

    routes_t = jnp.pad(routes.T, ((0, 6), (0, 0)))
    slot_inputs, slot_cotan, row_scale, slot_index = prep(
        q_arr, stream, out_grad, gain, routes_t, route_weight, experts, capacity
    )
    got_inputs = lax.all_to_all(slot_inputs, SP, 0, 0, tiled=True)
    slot_cotan, got_inputs = lax.optimization_barrier((slot_cotan, got_inputs))
    got_cotan = lax.all_to_all(slot_cotan, SP, 0, 0, tiled=True)

    low = shifted(got_inputs, "tp", 1)
    high = shifted(got_inputs, "tp", -1)
    far_top = shifted(low[:half], "tp", 1)
    far_bottom = shifted(high[half:], "tp", -1)
    rows = jnp.zeros((slots, model_width), BF)

    def put(buffer, value, row, k):
        return lax.dynamic_update_slice(buffer, value, (row, (k % 4) * width))

    rows = put(rows, got_inputs, 0, q)
    rows = put(rows, low, 0, q + 3)
    rows = put(rows, high, 0, q + 1)
    rows = put(rows, far_top, 0, q + 2)
    rows = put(rows, far_bottom, half, q + 2)

    hidden_parts = [contract(got_cotan, down_rel[j], 1, 1) for j in range(4)]
    hidden_grad = hidden_parts[0]
    for j in (1, 2, 3):
        hidden_grad = hidden_grad + shifted(hidden_parts[j].astype(BF), "tp", j).astype(F32)

    gate_pre = contract(rows, gate_w, 1, 0)
    up_pre = contract(rows, up_w, 1, 0)
    hidden = (jax.nn.silu(gate_pre) * up_pre).astype(BF)
    up_grad = (hidden_grad * jax.nn.silu(gate_pre)).astype(BF)
    gate_grad = (hidden_grad * up_pre * silu_grad(gate_pre)).astype(BF)

    def pair_block(k):
        return (
            contract(gate_grad, rows_of(gate_w, k), 1, 1)
            + contract(up_grad, rows_of(up_w, k), 1, 1)
        )

    far = pair_block(q + 2).astype(BF)
    go_top = shifted(far[:half], "tp", 1)
    go_bottom = shifted(far[half:], "tp", -1)
    next_block = pair_block(q + 1)
    prev_block = pair_block(q + 3)
    next_low = shifted(next_block[half:].astype(BF), "tp", 1)
    prev_low = shifted(prev_block[:half].astype(BF), "tp", -1)
    own = pair_block(q)
    next_sum = shifted((next_block[:half] + go_top.astype(F32)).astype(BF), "tp", 1)
    prev_sum = shifted((prev_block[half:] + go_bottom.astype(F32)).astype(BF), "tp", -1)
    summed = jnp.concatenate(
        [
            own[:half] + next_sum.astype(F32) + prev_low.astype(F32),
            own[half:] + next_low.astype(F32) + prev_sum.astype(F32),
        ]
    ).astype(BF)
    back = lax.all_to_all(summed, SP, 0, 0, tiled=True)

    gate_wgrad = contract(rows, gate_grad, 0, 0).astype(BF)
    up_wgrad = contract(rows, up_grad, 0, 0).astype(BF)

    hidden, summed = lax.optimization_barrier((hidden, summed))
    hidden_rel = [hidden] + [shifted(hidden, "tp", -j) for j in (1, 2, 3)]
    down_blocks = [contract(h, got_cotan, 0, 0).astype(BF) for h in hidden_rel]
    down_wgrad = jnp.zeros((units, model_width), BF)
    for j in range(4):
        block = down_blocks[j] if j == 0 else shifted(down_blocks[j], "tp", j)
        down_wgrad = put(down_wgrad, block, 0, q + 4 - j)

    scaled_grad, part_mean = combine(q_arr, back, slot_index, stream, row_scale, gain)
    totals = [part_mean] + [shifted(part_mean, "tp", j) for j in (1, 2, 3)]
    total_state = states[0] + states[1]
    gate_float = gate_branch.astype(F32)
    gelu_gate, gelu_back = jax.vjp(jax.nn.gelu, gate_float)
    gate_mul = gelu_back(total_state)[0]
    lru_out = (total_state * gelu_gate).astype(BF)
    lru_rel = jnp.concatenate(
        [lru_out] + [shifted(lru_out, "tp", -j) for j in (1, 2, 3)], axis=1
    )
    grad_b, *blocks = stream_back(q_arr, totals, scaled_grad, stream, out_grad, row_scale, proj_rel)
    lru_parts = [blocks[0]] + [shifted(blocks[j], "tp", j) for j in (1, 2, 3)]

    conv_float = conv_out.astype(F32)
    ones_row = jnp.ones((1, channels), F32)
    decays, direct, decay_mul, input_mul = [], [], [], []
    for d in range(2):
        decay_gate = jax.nn.sigmoid(contract(conv_out, decay_map[d, 0], 1, 0))
        input_gate = jax.nn.sigmoid(contract(conv_out, input_map[d, 0], 1, 0))
        decay_base = jax.nn.softplus(-decay_param[d])[None, :]
        log_decay = -rate_scale * decay_gate * decay_base + decay_shift[d]
        decay_rate = jnp.exp(log_decay)
        drive_scale = jnp.sqrt(-jnp.expm1(2.0 * log_decay))
        drive_term = drive_scale * input_gate * conv_float
        log_mul = (states[d] - drive_term) - (
            input_gate * conv_float * decay_rate * decay_rate / drive_scale
        )
        decays.append(decay_rate)
        direct.append(drive_scale * input_gate)
        decay_mul.append(log_mul * (-rate_scale * decay_base) * decay_gate * (1.0 - decay_gate))
        input_mul.append(drive_scale * conv_float * input_gate * (1.0 - input_gate))
    decay = jnp.stack(decays)
    shift = jnp.stack(
        [
            jnp.concatenate([decays[0][1:], ones_row]),
            jnp.concatenate([ones_row, decays[1][:-1]]),
        ]
    )
    gate_branch_grad, inner, reach, summary = scan_back(
        lru_parts, gate_mul, gelu_gate, decay, shift
    )
    level = jnp.stack([summary, shifted(summary, "sp_2", 1)])
    level = jnp.concatenate([level] + [shifted(level, "sp_1", -j) for j in (1, 2, 3)])
    gathered = [level] + [shifted(level, "sp_0", -j) for j in (1, 2, 3)]
    at = jnp.stack([z, y, c]).astype(jnp.int32)
    conv_grad = final_back(
        at,
        gathered,
        inner,
        reach,
        jnp.stack(direct),
        jnp.stack(decay_mul),
        jnp.stack(input_mul),
        decay_map[:, 0],
        input_map[:, 0],
    )

    partial = contract(grad_b, lru_rel, 0, 0).astype(BF)
    piece = partial.reshape(4, 2, width // 8, 4 * channels)
    keep = lax.dynamic_slice_in_dim(piece, c, 1, 1)[:, 0]
    give = lax.dynamic_slice_in_dim(piece, 1 - c, 1, 1)[:, 0]
    piece = keep.astype(F32) + shifted(give, "sp_2", 1).astype(F32)
    piece_b = piece.astype(BF)

    def run(array, k):
        return lax.dynamic_slice_in_dim(array, k % 4, 1, 0)[0]

    piece = run(piece, y)
    for j in (1, 2, 3):
        piece = piece + shifted(run(piece_b, y + j), "sp_1", j).astype(F32)
    piece_b = piece.astype(BF)
    out_proj_grad = 0.0
    for j in range(4):
        block = lax.dynamic_slice_in_dim(
            piece_b, ((z + j + 4 - q) % 4) * channels, channels, 1
        )
        moved = lax.ppermute(
            block,
            ("sp_0", "tp"),
            [(a * 4 + b, b * 4 + (a + j) % 4) for a in range(4) for b in range(4)],
        )
        out_proj_grad = out_proj_grad + moved.astype(F32)

    return (
        conv_grad,
        gate_branch_grad,
        out_proj_grad,
        gate_wgrad[None],
        up_wgrad[None],
        down_wgrad[None],
    )


def solution(mesh):
    torus = Mesh(mesh.devices.reshape(4, 4, 2, mesh.shape["tp"]), ("sp_0", "sp_1", "sp_2", "tp"))
    in_specs = (
        P(SP, None),
        P(SP, None),
        P(),
        P(SP, None),
        P(SP, None),
        P(SP, None, "tp"),
        P(SP, None, "tp"),
        P(SP, "tp", None),
        P(None, "tp"),
        P(SP, "tp"),
        P(SP, "tp"),
        P(None, "tp", None, None),
        P(None, "tp", None, None),
        P(None, "tp"),
        P(None, SP, "tp"),
        P(None, SP, "tp"),
    )
    out_specs = (
        P(SP, "tp"),
        P(SP, "tp"),
        P(SP, "tp"),
        P(SP, None, "tp"),
        P(SP, None, "tp"),
        P(SP, "tp", None),
    )
    return jax.shard_map(body, mesh=torus, in_specs=in_specs, out_specs=out_specs, check_vma=False)
```

```python
import functools

import jax
import jax.numpy as jnp
from jax import lax
from jax.experimental import pallas as pl
from jax.experimental.pallas import tpu as pltpu
from jax.sharding import Mesh
from jax.sharding import PartitionSpec as P


TOP = 2
SP = ("sp_0", "sp_1", "sp_2")
BF = jnp.bfloat16
F32 = jnp.float32

rate_scale = 8.0
norm_eps = 1e-06


def contract(left, right, left_dim, right_dim):
    return lax.dot_general(
        left, right, (((left_dim,), (right_dim,)), ((), ())), preferred_element_type=F32
    )


def shifted(x, axis, k):
    n = lax.axis_size(axis)
    return lax.ppermute(x, axis, [(i, (i + k) % n) for i in range(n)])


def exchanged(x):
    return lax.all_to_all(x, SP, 0, 0, tiled=True)


def vmem():
    return pl.BlockSpec(memory_space=pltpu.MemorySpace.VMEM)


def prep_kernel(
    q_ref, stream_ref, stream_q_ref, cotan_ref, gain_ref, routes_ref, weight_ref,
    inputs_ref, slots_ref, scale_ref, index_ref, *, experts, capacity,
):
    tokens, width = stream_ref.shape
    padded = -(-capacity // 8) * 8
    slots = experts * padded
    whole = stream_ref[...].astype(F32)
    scale = lax.rsqrt(jnp.sum(whole * whole, axis=1, keepdims=True) * (1.0 / width) + norm_eps)
    scale_ref[...] = scale
    normed = (stream_q_ref[...].astype(F32) * scale * gain_ref[...]).astype(BF)
    weight = jnp.concatenate([weight_ref[...]] * 64, axis=0).T
    expert = lax.broadcasted_iota(jnp.int32, (experts, tokens), 0)
    hits = [jnp.where(expert == routes_ref[k : k + 1, :], 1.0, 0.0) for k in range(TOP)]
    before = jnp.where(
        lax.broadcasted_iota(jnp.int32, (tokens, tokens), 0)
        < lax.broadcasted_iota(jnp.int32, (tokens, tokens), 1),
        1.0,
        0.0,
    ).astype(BF)
    earlier = jnp.dot((hits[0] + hits[1]).astype(BF), before, preferred_element_type=F32)
    place = lax.broadcasted_iota(jnp.int32, (slots, tokens), 0)
    picks = []
    for k in range(TOP):
        rank = jnp.sum(earlier * hits[k], axis=0, keepdims=True).astype(jnp.int32)
        slot = routes_ref[k : k + 1, :] * padded + rank
        index_ref[k : k + 1, :] = slot
        picks.append(jnp.where(place == slot, 1.0, 0.0))

    def store(out_ref, value):
        for e in range(experts):
            out_ref[e] = value[e * padded : e * padded + capacity].astype(BF)

    store(
        inputs_ref,
        jnp.dot((picks[0] + picks[1]).astype(BF), normed, preferred_element_type=F32),
    )
    cotan = cotan_ref[...].astype(F32)
    total = 0.0
    for k in range(TOP):
        scaled = (weight[:, k : k + 1] * cotan).astype(BF)
        total = total + jnp.dot(picks[k].astype(BF), scaled, preferred_element_type=F32)
    store(slots_ref, total)


def prep(q, stream, out_grad, gain, routes_t, weight, experts, capacity):
    tokens, width = stream.shape
    quarter = width // 4
    full = lambda shape: pl.BlockSpec(shape, lambda i, q_ref: (0, 0))
    part = lambda rows: pl.BlockSpec((rows, quarter), lambda i, q_ref: (0, q_ref[0]))
    return pl.pallas_call(
        functools.partial(prep_kernel, experts=experts, capacity=capacity),
        grid_spec=pltpu.PrefetchScalarGridSpec(
            num_scalar_prefetch=1,
            grid=(1,),
            in_specs=[
                full((tokens, width)),
                part(tokens),
                part(tokens),
                full((1, quarter)),
                full((TOP, tokens)),
                full((TOP, tokens)),
            ],
            out_specs=[
                pl.BlockSpec((experts, capacity, quarter), lambda i, q_ref: (0, 0, 0)),
                pl.BlockSpec((experts, capacity, quarter), lambda i, q_ref: (0, 0, 0)),
                full((tokens, 1)),
                full((8, tokens)),
            ],
        ),
        out_shape=[
            jax.ShapeDtypeStruct((experts, capacity, quarter), BF),
            jax.ShapeDtypeStruct((experts, capacity, quarter), BF),
            jax.ShapeDtypeStruct((tokens, 1), F32),
            jax.ShapeDtypeStruct((8, tokens), jnp.int32),
        ],
        name="prep",
    )(q, stream, stream, out_grad, gain, routes_t, weight)


def pair_sum_kernel(own_ref, a0_ref, a1_ref, b0_ref, b1_ref, out_ref, sum_ref):
    half = a0_ref.shape[0]
    sources, capacity, _ = out_ref.shape
    sum_ref[:half] = own_ref[:half] + (a0_ref[...].astype(F32) + a1_ref[...].astype(F32))
    sum_ref[half:] = own_ref[half:] + (b0_ref[...].astype(F32) + b1_ref[...].astype(F32))
    for e in range(sources):
        out_ref[e] = sum_ref[e * capacity : (e + 1) * capacity, :].astype(BF)


def pair_sum(own, top, bottom, sources):
    slots, width = own.shape
    return pl.pallas_call(
        pair_sum_kernel,
        in_specs=[vmem()] * 5,
        out_specs=vmem(),
        out_shape=jax.ShapeDtypeStruct((sources, slots // sources, width), BF),
        scratch_shapes=[pltpu.VMEM((slots, width), F32)],
        name="pair_sum",
    )(own, *top, *bottom)


def combine_kernel(
    q_ref, back_ref, index_ref, stream_ref, scale_ref, gain_ref, grad_ref, part_ref, rows_ref
):
    sources, capacity, quarter = back_ref.shape
    slots = rows_ref.shape[0]
    padded = slots // sources
    tokens = stream_ref.shape[0]
    for e in range(sources):
        rows_ref[e * padded : e * padded + padded, :] = jnp.concatenate(
            [back_ref[e].astype(F32), jnp.zeros((padded - capacity, quarter), F32)], axis=0
        )
    place = lax.broadcasted_iota(jnp.int32, (slots, tokens), 0)
    pick = jnp.where(
        (place == index_ref[0:1, :]) | (place == index_ref[1:2, :]), 1.0, 0.0
    ).astype(BF)
    normed_grad = lax.dot_general(
        pick, rows_ref[...].astype(BF), (((0,), (0,)), ((), ())), preferred_element_type=F32
    )
    scaled_grad = gain_ref[...] * normed_grad
    grad_ref[...] = scaled_grad
    unit = stream_ref[...].astype(F32) * scale_ref[...]
    part = jnp.sum(unit * scaled_grad, axis=1, keepdims=True)
    part_ref[...] = jnp.broadcast_to(part, (tokens, 128)).T[:8]


def combine(q, back, index, stream, scale, gain):
    sources, capacity, quarter = back.shape
    tokens = stream.shape[0]
    full = lambda shape: pl.BlockSpec(shape, lambda i, q_ref: (0, 0))
    return pl.pallas_call(
        combine_kernel,
        grid_spec=pltpu.PrefetchScalarGridSpec(
            num_scalar_prefetch=1,
            grid=(1,),
            in_specs=[
                pl.BlockSpec((sources, capacity, quarter), lambda i, q_ref: (0, 0, 0)),
                full((8, tokens)),
                pl.BlockSpec((tokens, quarter), lambda i, q_ref: (0, q_ref[0])),
                full((tokens, 1)),
                full((1, quarter)),
            ],
            out_specs=[full((tokens, quarter)), full((8, tokens))],
            scratch_shapes=[pltpu.VMEM((sources * (-(-capacity // 8) * 8), quarter), F32)],
        ),
        out_shape=[
            jax.ShapeDtypeStruct((tokens, quarter), F32),
            jax.ShapeDtypeStruct((8, tokens), F32),
        ],
        name="combine",
    )(q, back, index, stream, scale, gain)


def stream_kernel(
    q_ref, t0_ref, t1_ref, t2_ref, t3_ref, grad_ref, stream_ref, cotan_ref, scale_ref,
    p0_ref, p1_ref, p2_ref, p3_ref, sgb_ref, b0_ref, b1_ref, b2_ref, b3_ref, *, width,
):
    total = (t0_ref[...] + t1_ref[...]) + (t2_ref[...] + t3_ref[...])
    column = jnp.concatenate([total] * 16, axis=0).T[:, :1]
    mean = column * (1.0 / width)
    scale = scale_ref[...]
    unit = stream_ref[...].astype(F32) * scale
    grad = cotan_ref[...].astype(F32) + scale * (grad_ref[...] - unit * mean)
    grad_b = grad.astype(BF)
    lanes = sgb_ref.shape[2]
    for k in range(sgb_ref.shape[0]):
        sgb_ref[k] = grad_b[:, k * lanes : (k + 1) * lanes]
    for p_ref, b_ref in ((p1_ref, b1_ref), (p2_ref, b2_ref), (p3_ref, b3_ref), (p0_ref, b0_ref)):
        b_ref[...] = jnp.dot(grad_b, p_ref[...], preferred_element_type=F32).astype(b_ref.dtype)


def stream_back(q, totals, grad, stream, out_grad, scale, projs):
    tokens, quarter = grad.shape
    channels = projs[0].shape[1]
    full = lambda shape: pl.BlockSpec(shape, lambda i, q_ref: (0, 0))
    part = lambda rows: pl.BlockSpec((rows, quarter), lambda i, q_ref: (0, q_ref[0]))
    return pl.pallas_call(
        functools.partial(stream_kernel, width=stream.shape[1]),
        grid_spec=pltpu.PrefetchScalarGridSpec(
            num_scalar_prefetch=1,
            grid=(1,),
            in_specs=[full((8, tokens))] * 4
            + [full((tokens, quarter)), part(tokens), part(tokens), full((tokens, 1))]
            + [full((quarter, channels))] * 4,
            out_specs=[pl.BlockSpec((8, tokens, quarter // 8), lambda i, q_ref: (0, 0, 0))]
            + [full((tokens, channels))] * 4,
        ),
        out_shape=[jax.ShapeDtypeStruct((8, tokens, quarter // 8), BF)]
        + [jax.ShapeDtypeStruct((tokens, channels), F32)]
        + [jax.ShapeDtypeStruct((tokens, channels), BF)] * 3,
        name="stream_back",
    )(q, *totals, grad, stream, out_grad, scale, *projs)


def gather_columns_kernel(q_ref, b0_ref, b1_ref, b2_ref, b3_ref, out_ref):
    q = q_ref[0]
    width = b0_ref.shape[1]
    for j, b_ref in enumerate((b0_ref, b1_ref, b2_ref, b3_ref)):
        start = pl.multiple_of(lax.rem(q + 4 - j, 4) * width, width)
        out_ref[:, pl.ds(start, width)] = b_ref[...]


def gather_columns(q, blocks):
    rows, width = blocks[0].shape
    return pl.pallas_call(
        gather_columns_kernel,
        in_specs=[pl.BlockSpec(memory_space=pltpu.MemorySpace.SMEM)] + [vmem()] * 4,
        out_specs=vmem(),
        out_shape=jax.ShapeDtypeStruct((rows, 4 * width), BF),
        name="gather_columns",
    )(q, *blocks)


CHUNKS = 8


def scan_kernel(
    b0_ref, b1_ref, b2_ref, b3_ref, gate_mul_ref, gelu_ref, decay_ref, shift_ref,
    branch_ref, inner_ref, reach_ref, summary_ref, state_ref,
):
    tokens, channels = gelu_ref.shape
    length = tokens // CHUNKS
    out_grad = b0_ref[...] + (
        b1_ref[...].astype(F32) + b2_ref[...].astype(F32) + b3_ref[...].astype(F32)
    )
    branch_ref[...] = out_grad * gate_mul_ref[...]
    state_ref[...] = out_grad * gelu_ref[...]
    zero = jnp.zeros((CHUNKS, channels), F32)
    one = jnp.ones((CHUNKS, channels), F32)

    def step(i, carry):
        sum_0, mul_0, sum_1, mul_1 = carry
        at_0 = pl.ds(length - 1 - i, CHUNKS, stride=length)
        at_1 = pl.ds(i, CHUNKS, stride=length)
        coeff_0 = shift_ref[0, at_0, :]
        coeff_1 = shift_ref[1, at_1, :]
        sum_0 = state_ref[at_0, :] + coeff_0 * sum_0
        sum_1 = state_ref[at_1, :] + coeff_1 * sum_1
        mul_0 = coeff_0 * mul_0
        mul_1 = coeff_1 * mul_1
        inner_ref[0, at_0, :] = sum_0
        inner_ref[1, at_1, :] = sum_1
        reach_ref[0, at_0, :] = mul_0
        reach_ref[1, at_1, :] = mul_1
        return (sum_0, mul_0, sum_1, mul_1)

    lax.fori_loop(0, length, step, (zero, one, zero, one), unroll=4)
    row_sum = jnp.zeros((1, channels), F32)
    row_mul = jnp.ones((1, channels), F32)
    for s in reversed(range(CHUNKS)):
        at = s * length
        row_sum = inner_ref[0, at : at + 1, :] + reach_ref[0, at : at + 1, :] * row_sum
        row_mul = reach_ref[0, at : at + 1, :] * row_mul
    last = decay_ref[0, 0:1, :]
    summary_ref[0:1, :] = last * row_mul
    summary_ref[1:2, :] = last * row_sum
    row_sum = jnp.zeros((1, channels), F32)
    row_mul = jnp.ones((1, channels), F32)
    for s in range(CHUNKS):
        at = s * length + length - 1
        row_sum = inner_ref[1, at : at + 1, :] + reach_ref[1, at : at + 1, :] * row_sum
        row_mul = reach_ref[1, at : at + 1, :] * row_mul
    last = decay_ref[1, tokens - 1 : tokens, :]
    summary_ref[2:3, :] = last * row_mul
    summary_ref[3:4, :] = last * row_sum
    summary_ref[4:8, :] = jnp.zeros((4, channels), F32)


def scan_back(blocks, gate_mul, gelu_gate, decay, shift):
    tokens, channels = gelu_gate.shape
    lanes = 128
    flat = pl.BlockSpec((tokens, lanes), lambda i: (0, i))
    both = pl.BlockSpec((2, tokens, lanes), lambda i: (0, 0, i))
    return pl.pallas_call(
        scan_kernel,
        grid=(channels // lanes,),
        in_specs=[flat] * 6 + [both] * 2,
        out_specs=[flat, both, both, pl.BlockSpec((8, lanes), lambda i: (0, i))],
        out_shape=[
            jax.ShapeDtypeStruct((tokens, channels), F32),
            jax.ShapeDtypeStruct((2, tokens, channels), F32),
            jax.ShapeDtypeStruct((2, tokens, channels), F32),
            jax.ShapeDtypeStruct((8, channels), F32),
        ],
        scratch_shapes=[pltpu.VMEM((tokens, lanes), F32)],
        name="scan_back",
    )(*blocks, gate_mul, gelu_gate, decay, shift)


def split_dot(value, map_ref):
    high = value.astype(BF)
    low = (value - high.astype(F32)).astype(BF)
    dims = (((1,), (1,)), ((), ()))
    return lax.dot_general(high, map_ref, dims, preferred_element_type=F32) + lax.dot_general(
        low, map_ref, dims, preferred_element_type=F32
    )


def final_kernel(
    at_ref, g0_ref, g1_ref, g2_ref, g3_ref, inner_ref, reach_ref, direct_ref, decay_mul_ref,
    input_mul_ref, decay_map_ref, input_map_ref, out_ref, adjoint_ref,
):
    tokens, channels = out_ref.shape
    length = tokens // CHUNKS
    z, y, c = at_ref[0], at_ref[1], at_ref[2]
    mine = z * 8 + y * 2 + c
    refs = (g0_ref, g1_ref, g2_ref, g3_ref)
    from_right = jnp.zeros((1, channels), F32)
    from_left = jnp.zeros((1, channels), F32)

    def piece(k):
        dz = lax.rem(k // 8 - z + 4, 4)
        dy = lax.rem(lax.rem(k // 2, 4) - y + 4, 4)
        dc = lax.rem(lax.rem(k, 2) - c + 2, 2)
        row = dy * 2 + dc
        tile = jnp.where(dz == 0, refs[0][row], jnp.where(dz == 1, refs[1][row], jnp.where(dz == 2, refs[2][row], refs[3][row])))
        return tile

    for k in range(31):
        right = 31 - k
        tile = piece(right)
        from_right = jnp.where(right > mine, tile[1:2] + tile[0:1] * from_right, from_right)
        tile = piece(k)
        from_left = jnp.where(k < mine, tile[3:4] + tile[2:3] * from_left, from_left)
    carry = from_right
    for s in reversed(range(CHUNKS)):
        rows = slice(s * length, s * length + length)
        adjoint_ref[0, rows, :] = inner_ref[0, rows, :] + reach_ref[0, rows, :] * carry
        carry = adjoint_ref[0, s * length : s * length + 1, :]
    carry = from_left
    for s in range(CHUNKS):
        rows = slice(s * length, s * length + length)
        adjoint_ref[1, rows, :] = inner_ref[1, rows, :] + reach_ref[1, rows, :] * carry
        carry = adjoint_ref[1, s * length + length - 1 : s * length + length, :]
    total = jnp.zeros((tokens, channels), F32)
    for d in range(2):
        adjoint = adjoint_ref[d]
        total = total + adjoint * direct_ref[d]
        total = total + split_dot(adjoint * decay_mul_ref[d], decay_map_ref[d])
        total = total + split_dot(adjoint * input_mul_ref[d], input_map_ref[d])
    out_ref[...] = total


def final_back(at, gathered, inner, reach, direct, decay_mul, input_mul, decay_map, input_map):
    _, tokens, channels = inner.shape
    return pl.pallas_call(
        final_kernel,
        in_specs=[pl.BlockSpec(memory_space=pltpu.MemorySpace.SMEM)] + [vmem()] * 11,
        out_specs=vmem(),
        out_shape=jax.ShapeDtypeStruct((tokens, channels), F32),
        scratch_shapes=[pltpu.VMEM((2, tokens, channels), F32)],
        name="final_back",
    )(at, *gathered, inner, reach, direct, decay_mul, input_mul, decay_map, input_map)


def silu_grad(values):
    logistic = jax.nn.sigmoid(values)
    return logistic * (1.0 + values * (1.0 - logistic))


def body(
    out_grad,
    stream,
    norm_gain,
    routes,
    route_weight,
    gate_weight,
    up_weight,
    down_weight,
    out_proj,
    conv_out,
    gate_branch,
    decay_map,
    input_map,
    decay_param,
    decay_shift,
    states,
):
    sources = lax.axis_size(SP)
    experts = sources
    token_count, model_width = stream.shape
    capacity = (5 * TOP * token_count + 4 * experts - 1) // (4 * experts)
    slots = sources * capacity
    half = slots // 2
    width = model_width // 4
    q = lax.axis_index("tp")
    z, y, c = (lax.axis_index(a) for a in SP)
    q_arr = q.astype(jnp.int32).reshape(1)
    gate_w, up_w, down_w = gate_weight[0], up_weight[0], down_weight[0]
    channels = out_proj.shape[1]
    gain = lax.dynamic_slice_in_dim(norm_gain, q * width, width, 0).astype(F32)[None, :]

    def rows_of(array, k):
        return lax.dynamic_slice_in_dim(array, (k % 4) * width, width, 0)

    def cols_of(array, k):
        return lax.dynamic_slice_in_dim(array, (k % 4) * width, width, 1)

    down_rel = [cols_of(down_w, q)] + [
        shifted(cols_of(down_w, q + 4 - j), "tp", -j) for j in (1, 2, 3)
    ]
    proj_rel = [rows_of(out_proj, q)] + [
        shifted(rows_of(out_proj, q + 4 - j), "tp", -j) for j in (1, 2, 3)
    ]

    slot_inputs, slot_cotan, row_scale, slot_index = prep(
        q_arr, stream, out_grad, gain, routes.T, route_weight.T, experts, capacity
    )
    got_inputs = exchanged(slot_inputs).reshape(slots, width)
    got_cotan = exchanged(slot_cotan).reshape(slots, width)

    low = shifted(got_inputs, "tp", 1)
    high = shifted(got_inputs, "tp", -1)
    far_top = shifted(low[:half], "tp", 1)
    far_bottom = shifted(high[half:], "tp", -1)
    rows = jnp.zeros((slots, model_width), BF)

    def put(buffer, value, row, k):
        return lax.dynamic_update_slice(buffer, value, (row, (k % 4) * width))

    rows = put(rows, got_inputs, 0, q)
    rows = put(rows, low, 0, q + 3)
    rows = put(rows, high, 0, q + 1)
    rows = put(rows, far_top, 0, q + 2)
    rows = put(rows, far_bottom, half, q + 2)

    hidden_parts = [contract(got_cotan, down_rel[j], 1, 1) for j in range(4)]
    hidden_grad = hidden_parts[0]
    for j in (1, 2, 3):
        hidden_grad = hidden_grad + shifted(hidden_parts[j].astype(BF), "tp", j).astype(F32)

    gate_pre = contract(rows, gate_w, 1, 0)
    up_pre = contract(rows, up_w, 1, 0)
    hidden = (jax.nn.silu(gate_pre) * up_pre).astype(BF)
    up_grad = (hidden_grad * jax.nn.silu(gate_pre)).astype(BF)
    gate_grad = (hidden_grad * up_pre * silu_grad(gate_pre)).astype(BF)

    def pair_block(k):
        return (
            contract(gate_grad, rows_of(gate_w, k), 1, 1)
            + contract(up_grad, rows_of(up_w, k), 1, 1)
        )

    far = pair_block(q + 2).astype(BF)
    go_top = shifted(far[:half], "tp", 1)
    go_bottom = shifted(far[half:], "tp", -1)
    next_block = pair_block(q + 1)
    prev_block = pair_block(q + 3)
    next_low = shifted(next_block[half:].astype(BF), "tp", 1)
    prev_low = shifted(prev_block[:half].astype(BF), "tp", -1)
    own = pair_block(q)
    next_sum = shifted((next_block[:half] + go_top.astype(F32)).astype(BF), "tp", 1)
    prev_sum = shifted((prev_block[half:] + go_bottom.astype(F32)).astype(BF), "tp", -1)
    summed = pair_sum(own, (next_sum, prev_low), (next_low, prev_sum), sources)
    back = lax.all_to_all(summed, SP, 0, 0, tiled=True)

    gate_wgrad = contract(rows, gate_grad, 0, 0).astype(BF)
    up_wgrad = contract(rows, up_grad, 0, 0).astype(BF)

    hidden_rel = [hidden] + [shifted(hidden, "tp", -j) for j in (1, 2, 3)]
    down_blocks = [contract(h, got_cotan, 0, 0).astype(BF) for h in hidden_rel]
    down_parts = [shifted(down_blocks[j], "tp", j) for j in (1, 2, 3)]
    down_wgrad = gather_columns(q_arr, [down_blocks[0]] + down_parts)

    scaled_grad, part_mean = combine(q_arr, back, slot_index, stream, row_scale, gain)
    totals = [part_mean] + [shifted(part_mean, "tp", j) for j in (1, 2, 3)]
    total_state = states[0] + states[1]
    gate_float = gate_branch.astype(F32)
    gelu_gate, gelu_back = jax.vjp(jax.nn.gelu, gate_float)
    gate_mul = gelu_back(total_state)[0]
    lru_out = (total_state * gelu_gate).astype(BF)
    lru_rel = jnp.concatenate([lru_out] + [shifted(lru_out, "tp", -j) for j in (1, 2, 3)], axis=1)
    pair = [lru_rel, shifted(lru_rel, "sp_2", 1)]
    pair = jnp.where(c == 0, jnp.stack(pair), jnp.stack(pair[::-1]))
    lru_rows = jnp.zeros((4,) + pair.shape, BF)
    for j in range(4):
        block = pair if j == 0 else shifted(pair, "sp_1", -j)
        lru_rows = lax.dynamic_update_slice(lru_rows, block[None], ((y + j) % 4, 0, 0, 0))
    lru_rows = lru_rows.reshape(-1, 4 * channels)
    grad_b, *blocks = stream_back(
        q_arr, totals, scaled_grad, stream, out_grad, row_scale, proj_rel
    )
    lru_parts = [blocks[0]] + [shifted(blocks[j], "tp", j) for j in (1, 2, 3)]

    conv_float = conv_out.astype(F32)
    ones_row = jnp.ones((1, channels), F32)
    decays, direct, decay_mul, input_mul = [], [], [], []
    for d in range(2):
        decay_gate = jax.nn.sigmoid(contract(conv_out, decay_map[d, 0], 1, 0))
        input_gate = jax.nn.sigmoid(contract(conv_out, input_map[d, 0], 1, 0))
        decay_base = jax.nn.softplus(-decay_param[d])[None, :]
        log_decay = -rate_scale * decay_gate * decay_base + decay_shift[d]
        decay_rate = jnp.exp(log_decay)
        drive_scale = jnp.sqrt(-jnp.expm1(2.0 * log_decay))
        drive_term = drive_scale * input_gate * conv_float
        log_mul = (states[d] - drive_term) - (
            input_gate * conv_float * decay_rate * decay_rate / drive_scale
        )
        decays.append(decay_rate)
        direct.append(drive_scale * input_gate)
        decay_mul.append(log_mul * (-rate_scale * decay_base) * decay_gate * (1.0 - decay_gate))
        input_mul.append(drive_scale * conv_float * input_gate * (1.0 - input_gate))
    decay = jnp.stack(decays)
    shift = jnp.stack(
        [
            jnp.concatenate([decays[0][1:], ones_row]),
            jnp.concatenate([ones_row, decays[1][:-1]]),
        ]
    )
    gate_branch_grad, inner, reach, summary = scan_back(
        lru_parts, gate_mul, gelu_gate, decay, shift
    )
    level = jnp.stack([summary, shifted(summary, "sp_2", 1)])
    level = jnp.concatenate([level] + [shifted(level, "sp_1", -j) for j in (1, 2, 3)])
    gathered = [level] + [shifted(level, "sp_0", -j) for j in (1, 2, 3)]
    at = jnp.stack([z, y, c]).astype(jnp.int32)
    direct, decay_mul, input_mul = jnp.stack(direct), jnp.stack(decay_mul), jnp.stack(input_mul)
    conv_grad = final_back(
        at,
        gathered,
        inner,
        reach,
        direct,
        decay_mul,
        input_mul,
        decay_map[:, 0],
        input_map[:, 0],
    )

    grad_rows = lax.all_to_all(grad_b, ("sp_1", "sp_2"), 0, 0, tiled=True)
    piece_b = contract(grad_rows.reshape(-1, width // 8), lru_rows, 0, 0).astype(BF)
    out_proj_grad = 0.0
    for j in range(4):
        block = lax.dynamic_slice_in_dim(
            piece_b, ((z + j + 4 - q) % 4) * channels, channels, 1
        )
        moved = lax.ppermute(
            block,
            ("sp_0", "tp"),
            [(a * 4 + b, b * 4 + (a + j) % 4) for a in range(4) for b in range(4)],
        )
        out_proj_grad = out_proj_grad + moved.astype(F32)

    return (
        conv_grad,
        gate_branch_grad,
        out_proj_grad,
        gate_wgrad[None],
        up_wgrad[None],
        down_wgrad[None],
    )


def solution(mesh):
    torus = Mesh(mesh.devices.reshape(4, 4, 2, mesh.shape["tp"]), ("sp_0", "sp_1", "sp_2", "tp"))
    in_specs = (
        P(SP, None),
        P(SP, None),
        P(),
        P(SP, None),
        P(SP, None),
        P(SP, None, "tp"),
        P(SP, None, "tp"),
        P(SP, "tp", None),
        P(None, "tp"),
        P(SP, "tp"),
        P(SP, "tp"),
        P(None, "tp", None, None),
        P(None, "tp", None, None),
        P(None, "tp"),
        P(None, SP, "tp"),
        P(None, SP, "tp"),
    )
    out_specs = (
        P(SP, "tp"),
        P(SP, "tp"),
        P(SP, "tp"),
        P(SP, None, "tp"),
        P(SP, None, "tp"),
        P(SP, "tp", None),
    )
    return jax.shard_map(body, mesh=torus, in_specs=in_specs, out_specs=out_specs, check_vma=False)
```

```python
import functools

import jax
import jax.numpy as jnp
from jax import lax
from jax.experimental import pallas as pl
from jax.experimental.pallas import tpu as pltpu
from jax.sharding import Mesh
from jax.sharding import PartitionSpec as P


TOP = 2
SP = ("sp_0", "sp_1", "sp_2")
BF = jnp.bfloat16
F32 = jnp.float32

GRANT = pltpu.CompilerParams(vmem_limit_bytes=28 * 1024 * 1024)
rate_scale = 8.0
norm_eps = 1e-06


def contract(left, right, left_dim, right_dim):
    return lax.dot_general(
        left, right, (((left_dim,), (right_dim,)), ((), ())), preferred_element_type=F32
    )


def shifted(x, axis, k):
    n = lax.axis_size(axis)
    return lax.ppermute(x, axis, [(i, (i + k) % n) for i in range(n)])


def exchanged(x):
    return lax.all_to_all(x, SP, 0, 0, tiled=True)


def vmem():
    return pl.BlockSpec(memory_space=pltpu.MemorySpace.VMEM)


def prep_kernel(
    q_ref, stream_ref, stream_q_ref, cotan_ref, gain_ref, routes_ref, weight_ref,
    inputs_ref, slots_ref, scale_ref, index_ref, *, experts, capacity,
):
    tokens, width = stream_ref.shape
    padded = -(-capacity // 8) * 8
    slots = experts * padded
    whole = stream_ref[...].astype(F32)
    scale = lax.rsqrt(jnp.sum(whole * whole, axis=1, keepdims=True) * (1.0 / width) + norm_eps)
    scale_ref[...] = scale
    normed = (stream_q_ref[...].astype(F32) * scale * gain_ref[...]).astype(BF)
    weight = jnp.concatenate([weight_ref[...]] * 64, axis=0).T
    expert = lax.broadcasted_iota(jnp.int32, (experts, tokens), 0)
    hits = [jnp.where(expert == routes_ref[k : k + 1, :], 1.0, 0.0) for k in range(TOP)]
    before = jnp.where(
        lax.broadcasted_iota(jnp.int32, (tokens, tokens), 0)
        < lax.broadcasted_iota(jnp.int32, (tokens, tokens), 1),
        1.0,
        0.0,
    ).astype(BF)
    earlier = jnp.dot((hits[0] + hits[1]).astype(BF), before, preferred_element_type=F32)
    place = lax.broadcasted_iota(jnp.int32, (slots, tokens), 0)
    picks = []
    for k in range(TOP):
        rank = jnp.sum(earlier * hits[k], axis=0, keepdims=True).astype(jnp.int32)
        slot = routes_ref[k : k + 1, :] * padded + rank
        index_ref[k : k + 1, :] = slot
        picks.append(jnp.where(place == slot, 1.0, 0.0))

    def store(out_ref, value):
        for e in range(experts):
            out_ref[e] = value[e * padded : e * padded + capacity].astype(BF)

    store(
        inputs_ref,
        jnp.dot((picks[0] + picks[1]).astype(BF), normed, preferred_element_type=F32),
    )
    cotan = cotan_ref[...].astype(F32)
    total = 0.0
    for k in range(TOP):
        scaled = (weight[:, k : k + 1] * cotan).astype(BF)
        total = total + jnp.dot(picks[k].astype(BF), scaled, preferred_element_type=F32)
    store(slots_ref, total)


def prep(q, stream, out_grad, gain, routes_t, weight, experts, capacity):
    tokens, width = stream.shape
    quarter = width // 4
    full = lambda shape: pl.BlockSpec(shape, lambda i, q_ref: (0, 0))
    part = lambda rows: pl.BlockSpec((rows, quarter), lambda i, q_ref: (0, q_ref[0]))
    return pl.pallas_call(
        functools.partial(prep_kernel, experts=experts, capacity=capacity),
        grid_spec=pltpu.PrefetchScalarGridSpec(
            num_scalar_prefetch=1,
            grid=(1,),
            in_specs=[
                full((tokens, width)),
                part(tokens),
                part(tokens),
                full((1, quarter)),
                full((TOP, tokens)),
                full((TOP, tokens)),
            ],
            out_specs=[
                pl.BlockSpec((experts, capacity, quarter), lambda i, q_ref: (0, 0, 0)),
                pl.BlockSpec((experts, capacity, quarter), lambda i, q_ref: (0, 0, 0)),
                full((tokens, 1)),
                full((8, tokens)),
            ],
        ),
        out_shape=[
            jax.ShapeDtypeStruct((experts, capacity, quarter), BF),
            jax.ShapeDtypeStruct((experts, capacity, quarter), BF),
            jax.ShapeDtypeStruct((tokens, 1), F32),
            jax.ShapeDtypeStruct((8, tokens), jnp.int32),
        ],
        name="prep", compiler_params=GRANT,
    )(q, stream, stream, out_grad, gain, routes_t, weight)


def pair_sum_kernel(own_ref, a0_ref, a1_ref, b0_ref, b1_ref, out_ref, sum_ref):
    half = a0_ref.shape[0]
    sources, capacity, _ = out_ref.shape
    sum_ref[:half] = own_ref[:half] + (a0_ref[...].astype(F32) + a1_ref[...].astype(F32))
    sum_ref[half:] = own_ref[half:] + (b0_ref[...].astype(F32) + b1_ref[...].astype(F32))
    for e in range(sources):
        out_ref[e] = sum_ref[e * capacity : (e + 1) * capacity, :].astype(BF)


def pair_sum(own, top, bottom, sources):
    slots, width = own.shape
    return pl.pallas_call(
        pair_sum_kernel,
        in_specs=[vmem()] * 5,
        out_specs=vmem(),
        out_shape=jax.ShapeDtypeStruct((sources, slots // sources, width), BF),
        scratch_shapes=[pltpu.VMEM((slots, width), F32)],
        name="pair_sum", compiler_params=GRANT,
    )(own, *top, *bottom)


def combine_kernel(
    q_ref, back_ref, index_ref, stream_ref, scale_ref, gain_ref, grad_ref, part_ref, rows_ref
):
    sources, capacity, quarter = back_ref.shape
    slots = rows_ref.shape[0]
    padded = slots // sources
    tokens = stream_ref.shape[0]
    for e in range(sources):
        rows_ref[e * padded : e * padded + padded, :] = jnp.concatenate(
            [back_ref[e].astype(F32), jnp.zeros((padded - capacity, quarter), F32)], axis=0
        )
    place = lax.broadcasted_iota(jnp.int32, (slots, tokens), 0)
    pick = jnp.where(
        (place == index_ref[0:1, :]) | (place == index_ref[1:2, :]), 1.0, 0.0
    ).astype(BF)
    normed_grad = lax.dot_general(
        pick, rows_ref[...].astype(BF), (((0,), (0,)), ((), ())), preferred_element_type=F32
    )
    scaled_grad = gain_ref[...] * normed_grad
    grad_ref[...] = scaled_grad
    unit = stream_ref[...].astype(F32) * scale_ref[...]
    part = jnp.sum(unit * scaled_grad, axis=1, keepdims=True)
    part_ref[...] = jnp.broadcast_to(part, (tokens, 128)).T[:8]


def combine(q, back, index, stream, scale, gain):
    sources, capacity, quarter = back.shape
    tokens = stream.shape[0]
    full = lambda shape: pl.BlockSpec(shape, lambda i, q_ref: (0, 0))
    return pl.pallas_call(
        combine_kernel,
        grid_spec=pltpu.PrefetchScalarGridSpec(
            num_scalar_prefetch=1,
            grid=(1,),
            in_specs=[
                pl.BlockSpec((sources, capacity, quarter), lambda i, q_ref: (0, 0, 0)),
                full((8, tokens)),
                pl.BlockSpec((tokens, quarter), lambda i, q_ref: (0, q_ref[0])),
                full((tokens, 1)),
                full((1, quarter)),
            ],
            out_specs=[full((tokens, quarter)), full((8, tokens))],
            scratch_shapes=[pltpu.VMEM((sources * (-(-capacity // 8) * 8), quarter), F32)],
        ),
        out_shape=[
            jax.ShapeDtypeStruct((tokens, quarter), F32),
            jax.ShapeDtypeStruct((8, tokens), F32),
        ],
        name="combine", compiler_params=GRANT,
    )(q, back, index, stream, scale, gain)


def stream_kernel(
    q_ref, t0_ref, t1_ref, t2_ref, t3_ref, grad_ref, stream_ref, cotan_ref, scale_ref,
    p0_ref, p1_ref, p2_ref, p3_ref, sgb_ref, b0_ref, b1_ref, b2_ref, b3_ref, *, width,
):
    total = (t0_ref[...] + t1_ref[...]) + (t2_ref[...] + t3_ref[...])
    column = jnp.concatenate([total] * 16, axis=0).T[:, :1]
    mean = column * (1.0 / width)
    scale = scale_ref[...]
    unit = stream_ref[...].astype(F32) * scale
    grad = cotan_ref[...].astype(F32) + scale * (grad_ref[...] - unit * mean)
    grad_b = grad.astype(BF)
    lanes = sgb_ref.shape[2]
    for k in range(sgb_ref.shape[0]):
        sgb_ref[k] = grad_b[:, k * lanes : (k + 1) * lanes]
    for p_ref, b_ref in ((p1_ref, b1_ref), (p2_ref, b2_ref), (p3_ref, b3_ref), (p0_ref, b0_ref)):
        b_ref[...] = jnp.dot(grad_b, p_ref[...], preferred_element_type=F32).astype(b_ref.dtype)


def stream_back(q, totals, grad, stream, out_grad, scale, projs):
    tokens, quarter = grad.shape
    channels = projs[0].shape[1]
    full = lambda shape: pl.BlockSpec(shape, lambda i, q_ref: (0, 0))
    part = lambda rows: pl.BlockSpec((rows, quarter), lambda i, q_ref: (0, q_ref[0]))
    return pl.pallas_call(
        functools.partial(stream_kernel, width=stream.shape[1]),
        grid_spec=pltpu.PrefetchScalarGridSpec(
            num_scalar_prefetch=1,
            grid=(1,),
            in_specs=[full((8, tokens))] * 4
            + [full((tokens, quarter)), part(tokens), part(tokens), full((tokens, 1))]
            + [full((quarter, channels))] * 4,
            out_specs=[pl.BlockSpec((8, tokens, quarter // 8), lambda i, q_ref: (0, 0, 0))]
            + [full((tokens, channels))] * 4,
        ),
        out_shape=[jax.ShapeDtypeStruct((8, tokens, quarter // 8), BF)]
        + [jax.ShapeDtypeStruct((tokens, channels), F32)]
        + [jax.ShapeDtypeStruct((tokens, channels), BF)] * 3,
        name="stream_back", compiler_params=GRANT,
    )(q, *totals, grad, stream, out_grad, scale, *projs)


def gather_columns_kernel(q_ref, b0_ref, b1_ref, b2_ref, b3_ref, out_ref):
    q = q_ref[0]
    width = b0_ref.shape[1]
    for j, b_ref in enumerate((b0_ref, b1_ref, b2_ref, b3_ref)):
        start = pl.multiple_of(lax.rem(q + 4 - j, 4) * width, width)
        out_ref[:, pl.ds(start, width)] = b_ref[...]


def gather_columns(q, blocks):
    rows, width = blocks[0].shape
    return pl.pallas_call(
        gather_columns_kernel,
        in_specs=[pl.BlockSpec(memory_space=pltpu.MemorySpace.SMEM)] + [vmem()] * 4,
        out_specs=vmem(),
        out_shape=jax.ShapeDtypeStruct((rows, 4 * width), BF),
        name="gather_columns", compiler_params=GRANT,
    )(q, *blocks)


CHUNKS = 8


def scan_kernel(
    b0_ref, b1_ref, b2_ref, b3_ref, gate_mul_ref, gelu_ref, decay_ref, shift_ref,
    branch_ref, inner_ref, reach_ref, summary_ref, state_ref,
):
    tokens, channels = gelu_ref.shape
    length = tokens // CHUNKS
    out_grad = b0_ref[...] + (
        b1_ref[...].astype(F32) + b2_ref[...].astype(F32) + b3_ref[...].astype(F32)
    )
    branch_ref[...] = out_grad * gate_mul_ref[...]
    state_ref[...] = out_grad * gelu_ref[...]
    zero = jnp.zeros((CHUNKS, channels), F32)
    one = jnp.ones((CHUNKS, channels), F32)

    def step(i, carry):
        sum_0, mul_0, sum_1, mul_1 = carry
        at_0 = pl.ds(length - 1 - i, CHUNKS, stride=length)
        at_1 = pl.ds(i, CHUNKS, stride=length)
        coeff_0 = shift_ref[0, at_0, :]
        coeff_1 = shift_ref[1, at_1, :]
        sum_0 = state_ref[at_0, :] + coeff_0 * sum_0
        sum_1 = state_ref[at_1, :] + coeff_1 * sum_1
        mul_0 = coeff_0 * mul_0
        mul_1 = coeff_1 * mul_1
        inner_ref[0, at_0, :] = sum_0
        inner_ref[1, at_1, :] = sum_1
        reach_ref[0, at_0, :] = mul_0
        reach_ref[1, at_1, :] = mul_1
        return (sum_0, mul_0, sum_1, mul_1)

    lax.fori_loop(0, length, step, (zero, one, zero, one), unroll=4)
    row_sum = jnp.zeros((1, channels), F32)
    row_mul = jnp.ones((1, channels), F32)
    for s in reversed(range(CHUNKS)):
        at = s * length
        row_sum = inner_ref[0, at : at + 1, :] + reach_ref[0, at : at + 1, :] * row_sum
        row_mul = reach_ref[0, at : at + 1, :] * row_mul
    last = decay_ref[0, 0:1, :]
    summary_ref[0:1, :] = last * row_mul
    summary_ref[1:2, :] = last * row_sum
    row_sum = jnp.zeros((1, channels), F32)
    row_mul = jnp.ones((1, channels), F32)
    for s in range(CHUNKS):
        at = s * length + length - 1
        row_sum = inner_ref[1, at : at + 1, :] + reach_ref[1, at : at + 1, :] * row_sum
        row_mul = reach_ref[1, at : at + 1, :] * row_mul
    last = decay_ref[1, tokens - 1 : tokens, :]
    summary_ref[2:3, :] = last * row_mul
    summary_ref[3:4, :] = last * row_sum
    summary_ref[4:8, :] = jnp.zeros((4, channels), F32)


def scan_back(blocks, gate_mul, gelu_gate, decay, shift):
    tokens, channels = gelu_gate.shape
    lanes = 128
    flat = pl.BlockSpec((tokens, lanes), lambda i: (0, i))
    both = pl.BlockSpec((2, tokens, lanes), lambda i: (0, 0, i))
    return pl.pallas_call(
        scan_kernel,
        grid=(channels // lanes,),
        in_specs=[flat] * 6 + [both] * 2,
        out_specs=[flat, both, both, pl.BlockSpec((8, lanes), lambda i: (0, i))],
        out_shape=[
            jax.ShapeDtypeStruct((tokens, channels), F32),
            jax.ShapeDtypeStruct((2, tokens, channels), F32),
            jax.ShapeDtypeStruct((2, tokens, channels), F32),
            jax.ShapeDtypeStruct((8, channels), F32),
        ],
        scratch_shapes=[pltpu.VMEM((tokens, lanes), F32)],
        name="scan_back", compiler_params=GRANT,
    )(*blocks, gate_mul, gelu_gate, decay, shift)


def split_dot(value, map_ref):
    high = value.astype(BF)
    low = (value - high.astype(F32)).astype(BF)
    dims = (((1,), (1,)), ((), ()))
    return lax.dot_general(high, map_ref, dims, preferred_element_type=F32) + lax.dot_general(
        low, map_ref, dims, preferred_element_type=F32
    )


def final_kernel(
    at_ref, g0_ref, g1_ref, g2_ref, g3_ref, inner_ref, reach_ref, direct_ref, decay_mul_ref,
    input_mul_ref, decay_map_ref, input_map_ref, out_ref, adjoint_ref,
):
    tokens, channels = out_ref.shape
    length = tokens // CHUNKS
    z, y, c = at_ref[0], at_ref[1], at_ref[2]
    mine = z * 8 + y * 2 + c
    refs = (g0_ref, g1_ref, g2_ref, g3_ref)
    from_right = jnp.zeros((1, channels), F32)
    from_left = jnp.zeros((1, channels), F32)

    def piece(k):
        dz = lax.rem(k // 8 - z + 4, 4)
        dy = lax.rem(lax.rem(k // 2, 4) - y + 4, 4)
        dc = lax.rem(lax.rem(k, 2) - c + 2, 2)
        row = dy * 2 + dc
        tile = jnp.where(dz == 0, refs[0][row], jnp.where(dz == 1, refs[1][row], jnp.where(dz == 2, refs[2][row], refs[3][row])))
        return tile

    for k in range(31):
        right = 31 - k
        tile = piece(right)
        from_right = jnp.where(right > mine, tile[1:2] + tile[0:1] * from_right, from_right)
        tile = piece(k)
        from_left = jnp.where(k < mine, tile[3:4] + tile[2:3] * from_left, from_left)
    carry = from_right
    for s in reversed(range(CHUNKS)):
        rows = slice(s * length, s * length + length)
        adjoint_ref[0, rows, :] = inner_ref[0, rows, :] + reach_ref[0, rows, :] * carry
        carry = adjoint_ref[0, s * length : s * length + 1, :]
    carry = from_left
    for s in range(CHUNKS):
        rows = slice(s * length, s * length + length)
        adjoint_ref[1, rows, :] = inner_ref[1, rows, :] + reach_ref[1, rows, :] * carry
        carry = adjoint_ref[1, s * length + length - 1 : s * length + length, :]
    total = jnp.zeros((tokens, channels), F32)
    for d in range(2):
        adjoint = adjoint_ref[d]
        total = total + adjoint * direct_ref[d]
        total = total + split_dot(adjoint * decay_mul_ref[d], decay_map_ref[d])
        total = total + split_dot(adjoint * input_mul_ref[d], input_map_ref[d])
    out_ref[...] = total


def final_back(at, gathered, inner, reach, direct, decay_mul, input_mul, decay_map, input_map):
    _, tokens, channels = inner.shape
    return pl.pallas_call(
        final_kernel,
        in_specs=[pl.BlockSpec(memory_space=pltpu.MemorySpace.SMEM)] + [vmem()] * 11,
        out_specs=vmem(),
        out_shape=jax.ShapeDtypeStruct((tokens, channels), F32),
        scratch_shapes=[pltpu.VMEM((2, tokens, channels), F32)],
        name="final_back", compiler_params=GRANT,
    )(at, *gathered, inner, reach, direct, decay_mul, input_mul, decay_map, input_map)


def silu_grad(values):
    logistic = jax.nn.sigmoid(values)
    return logistic * (1.0 + values * (1.0 - logistic))


def body(
    out_grad,
    stream,
    norm_gain,
    routes,
    route_weight,
    gate_weight,
    up_weight,
    down_weight,
    out_proj,
    conv_out,
    gate_branch,
    decay_map,
    input_map,
    decay_param,
    decay_shift,
    states,
):
    sources = lax.axis_size(SP)
    experts = sources
    token_count, model_width = stream.shape
    capacity = (5 * TOP * token_count + 4 * experts - 1) // (4 * experts)
    slots = sources * capacity
    half = slots // 2
    width = model_width // 4
    q = lax.axis_index("tp")
    z, y, c = (lax.axis_index(a) for a in SP)
    q_arr = q.astype(jnp.int32).reshape(1)
    gate_w, up_w, down_w = gate_weight[0], up_weight[0], down_weight[0]
    channels = out_proj.shape[1]
    gain = lax.dynamic_slice_in_dim(norm_gain, q * width, width, 0).astype(F32)[None, :]

    def rows_of(array, k):
        return lax.dynamic_slice_in_dim(array, (k % 4) * width, width, 0)

    def cols_of(array, k):
        return lax.dynamic_slice_in_dim(array, (k % 4) * width, width, 1)

    down_rel = [cols_of(down_w, q)] + [
        shifted(cols_of(down_w, q + 4 - j), "tp", -j) for j in (1, 2, 3)
    ]
    proj_rel = [rows_of(out_proj, q)] + [
        shifted(rows_of(out_proj, q + 4 - j), "tp", -j) for j in (1, 2, 3)
    ]

    slot_inputs, slot_cotan, row_scale, slot_index = prep(
        q_arr, stream, out_grad, gain, routes.T, route_weight.T, experts, capacity
    )
    got_inputs = exchanged(slot_inputs).reshape(slots, width)
    got_cotan = exchanged(slot_cotan).reshape(slots, width)

    low = shifted(got_inputs, "tp", 1)
    high = shifted(got_inputs, "tp", -1)
    far_top = shifted(low[:half], "tp", 1)
    far_bottom = shifted(high[half:], "tp", -1)
    rows = jnp.zeros((slots, model_width), BF)

    def put(buffer, value, row, k):
        return lax.dynamic_update_slice(buffer, value, (row, (k % 4) * width))

    rows = put(rows, got_inputs, 0, q)
    rows = put(rows, low, 0, q + 3)
    rows = put(rows, high, 0, q + 1)
    rows = put(rows, far_top, 0, q + 2)
    rows = put(rows, far_bottom, half, q + 2)

    hidden_parts = [contract(got_cotan, down_rel[j], 1, 1) for j in range(4)]
    hidden_grad = hidden_parts[0]
    for j in (1, 2, 3):
        hidden_grad = hidden_grad + shifted(hidden_parts[j].astype(BF), "tp", j).astype(F32)

    gate_pre = contract(rows, gate_w, 1, 0)
    up_pre = contract(rows, up_w, 1, 0)
    hidden = (jax.nn.silu(gate_pre) * up_pre).astype(BF)
    up_grad = (hidden_grad * jax.nn.silu(gate_pre)).astype(BF)
    gate_grad = (hidden_grad * up_pre * silu_grad(gate_pre)).astype(BF)

    def pair_block(k):
        return (
            contract(gate_grad, rows_of(gate_w, k), 1, 1)
            + contract(up_grad, rows_of(up_w, k), 1, 1)
        )

    far = pair_block(q + 2).astype(BF)
    go_top = shifted(far[:half], "tp", 1)
    go_bottom = shifted(far[half:], "tp", -1)
    next_block = pair_block(q + 1)
    prev_block = pair_block(q + 3)
    next_low = shifted(next_block[half:].astype(BF), "tp", 1)
    prev_low = shifted(prev_block[:half].astype(BF), "tp", -1)
    own = pair_block(q)
    next_sum = shifted((next_block[:half] + go_top.astype(F32)).astype(BF), "tp", 1)
    prev_sum = shifted((prev_block[half:] + go_bottom.astype(F32)).astype(BF), "tp", -1)
    summed = pair_sum(own, (next_sum, prev_low), (next_low, prev_sum), sources)
    back = lax.all_to_all(summed, SP, 0, 0, tiled=True)

    gate_wgrad = contract(rows, gate_grad, 0, 0).astype(BF)
    up_wgrad = contract(rows, up_grad, 0, 0).astype(BF)

    hidden_rel = [hidden] + [shifted(hidden, "tp", -j) for j in (1, 2, 3)]
    down_blocks = [contract(h, got_cotan, 0, 0).astype(BF) for h in hidden_rel]
    down_parts = [shifted(down_blocks[j], "tp", j) for j in (1, 2, 3)]
    down_wgrad = gather_columns(q_arr, [down_blocks[0]] + down_parts)

    scaled_grad, part_mean = combine(q_arr, back, slot_index, stream, row_scale, gain)
    totals = [part_mean] + [shifted(part_mean, "tp", j) for j in (1, 2, 3)]
    total_state = states[0] + states[1]
    gate_float = gate_branch.astype(F32)
    gelu_gate, gelu_back = jax.vjp(jax.nn.gelu, gate_float)
    gate_mul = gelu_back(total_state)[0]
    lru_out = (total_state * gelu_gate).astype(BF)
    lru_rel = jnp.concatenate([lru_out] + [shifted(lru_out, "tp", -j) for j in (1, 2, 3)], axis=1)
    pair = [lru_rel, shifted(lru_rel, "sp_2", 1)]
    pair = jnp.where(c == 0, jnp.stack(pair), jnp.stack(pair[::-1]))
    lru_rows = jnp.zeros((4,) + pair.shape, BF)
    for j in range(4):
        block = pair if j == 0 else shifted(pair, "sp_1", -j)
        lru_rows = lax.dynamic_update_slice(lru_rows, block[None], ((y + j) % 4, 0, 0, 0))
    lru_rows = lru_rows.reshape(-1, 4 * channels)
    grad_b, *blocks = stream_back(
        q_arr, totals, scaled_grad, stream, out_grad, row_scale, proj_rel
    )
    lru_parts = [blocks[0]] + [shifted(blocks[j], "tp", j) for j in (1, 2, 3)]

    conv_float = conv_out.astype(F32)
    ones_row = jnp.ones((1, channels), F32)
    decays, direct, decay_mul, input_mul = [], [], [], []
    for d in range(2):
        decay_gate = jax.nn.sigmoid(contract(conv_out, decay_map[d, 0], 1, 0))
        input_gate = jax.nn.sigmoid(contract(conv_out, input_map[d, 0], 1, 0))
        decay_base = jax.nn.softplus(-decay_param[d])[None, :]
        log_decay = -rate_scale * decay_gate * decay_base + decay_shift[d]
        decay_rate = jnp.exp(log_decay)
        drive_scale = jnp.sqrt(-jnp.expm1(2.0 * log_decay))
        drive_term = drive_scale * input_gate * conv_float
        log_mul = (states[d] - drive_term) - (
            input_gate * conv_float * decay_rate * decay_rate / drive_scale
        )
        decays.append(decay_rate)
        direct.append(drive_scale * input_gate)
        decay_mul.append(log_mul * (-rate_scale * decay_base) * decay_gate * (1.0 - decay_gate))
        input_mul.append(drive_scale * conv_float * input_gate * (1.0 - input_gate))
    decay = jnp.stack(decays)
    shift = jnp.stack(
        [
            jnp.concatenate([decays[0][1:], ones_row]),
            jnp.concatenate([ones_row, decays[1][:-1]]),
        ]
    )
    gate_branch_grad, inner, reach, summary = scan_back(
        lru_parts, gate_mul, gelu_gate, decay, shift
    )
    level = jnp.stack([summary, shifted(summary, "sp_2", 1)])
    level = jnp.concatenate([level] + [shifted(level, "sp_1", -j) for j in (1, 2, 3)])
    gathered = [level] + [shifted(level, "sp_0", -j) for j in (1, 2, 3)]
    at = jnp.stack([z, y, c]).astype(jnp.int32)
    direct, decay_mul, input_mul = jnp.stack(direct), jnp.stack(decay_mul), jnp.stack(input_mul)
    conv_grad = final_back(
        at,
        gathered,
        inner,
        reach,
        direct,
        decay_mul,
        input_mul,
        decay_map[:, 0],
        input_map[:, 0],
    )

    grad_rows = lax.all_to_all(grad_b, ("sp_1", "sp_2"), 0, 0, tiled=True)
    piece_b = contract(grad_rows.reshape(-1, width // 8), lru_rows, 0, 0).astype(BF)
    out_proj_grad = 0.0
    for j in range(4):
        block = lax.dynamic_slice_in_dim(
            piece_b, ((z + j + 4 - q) % 4) * channels, channels, 1
        )
        moved = lax.ppermute(
            block,
            ("sp_0", "tp"),
            [(a * 4 + b, b * 4 + (a + j) % 4) for a in range(4) for b in range(4)],
        )
        out_proj_grad = out_proj_grad + moved.astype(F32)

    return (
        conv_grad,
        gate_branch_grad,
        out_proj_grad,
        gate_wgrad[None],
        up_wgrad[None],
        down_wgrad[None],
    )


def solution(mesh):
    torus = Mesh(mesh.devices.reshape(4, 4, 2, mesh.shape["tp"]), ("sp_0", "sp_1", "sp_2", "tp"))
    in_specs = (
        P(SP, None),
        P(SP, None),
        P(),
        P(SP, None),
        P(SP, None),
        P(SP, None, "tp"),
        P(SP, None, "tp"),
        P(SP, "tp", None),
        P(None, "tp"),
        P(SP, "tp"),
        P(SP, "tp"),
        P(None, "tp", None, None),
        P(None, "tp", None, None),
        P(None, "tp"),
        P(None, SP, "tp"),
        P(None, SP, "tp"),
    )
    out_specs = (
        P(SP, "tp"),
        P(SP, "tp"),
        P(SP, "tp"),
        P(SP, None, "tp"),
        P(SP, None, "tp"),
        P(SP, "tp", None),
    )
    return jax.shard_map(body, mesh=torus, in_specs=in_specs, out_specs=out_specs, check_vma=False)
```
